32 devices in a mesh: grp: 2 (over y), ep: 4 (over z), tp: 4 (over x, core).
Axes of the slice: x: 2, y: 2, z: 4, core: 2. Of those that a mesh axis runs over, the one named last changes fastest.
Arguments:
- queries: bfloat16 [1024, 1024], P(('grp', 'ep'), 'tp'), parts along dimension 0, may hold values from -6 to 6
- keys: bfloat16 [1024, 1024], P(('grp', 'ep'), 'tp'), parts along dimension 0, may hold values from -6 to 6
- values: bfloat16 [1024, 1024], P(('grp', 'ep'), 'tp'), parts along dimension 0, may hold values from -6 to 6
- lambdas: float32 [8], P('tp'), may hold values from 0.3 to 0.8
- head_gain: float32 [128], replicated, may hold values from 0.1 to 1.9
- tokens: bfloat16 [2048, 1536], P(('grp', 'ep')), parts along dimension 0, may hold values from -6 to 6
- route_ids: int32 [2048, 2], P(('grp', 'ep')), parts along dimension 0, may hold values from 0 to 3, all different within a row; in each aligned block of 256 rows (0 to 255, 256 to 511, ...) at most 256 rows name the same one
- route_weights: float32 [2048, 2], P(('grp', 'ep')), parts along dimension 0, may hold values from 0.2 to 1
- moe_gain: float32 [1536], replicated, may hold values from 0.1 to 1.9
- w_gate: bfloat16 [4, 1536, 3072], P('ep', None, 'tp'), may hold values from -0.15625 to 0.15625
- w_up: bfloat16 [4, 1536, 3072], P('ep', None, 'tp'), may hold values from -0.15625 to 0.15625
- w_down: bfloat16 [4, 3072, 1536], P('ep', 'tp'), may hold values from -0.109375 to 0.109375
Outputs:
- heads_out: bfloat16 [1024, 1024], P(('grp', 'ep'), 'tp'), parts along dimension 0
- expert_out: bfloat16 [2048, 1536], P(('grp', 'ep'), 'tp'), parts along dimension 0
The draws below stay inside these ranges and needn't reach their ends.
There are 2 independent parts, one for each index of `grp`. The reference program is written for one: setup_inputs(seed, part) draws one part's arguments, and reference() takes and returns one part's arrays. A program takes and returns all parts, laid end to end along the dimension named above; an argument that names none is the same for every part. Nothing has to cross between parts.
Inputs may be any that keep to these rules, and one draw needn't show every extreme that they name: `route_ids`: each row names 2 different experts. In the 256 rows of one device no expert is named more than 256 times, and in every draw some device names some expert exactly 256 times.
All inputs are finite; a program needn't handle non-finite values.
Results may differ from the reference program's by a relative error of at most 0.015.
Values may be sent and summed in bfloat16 or wider, within the bound.
A program may use at most 64 MiB of HBM per device.

```python
import math
import jax
import jax.numpy as jnp
import numpy as np
from jax import lax

D = 1536
FF = 3072
HEADS = 8
HEAD_DIM = 64
VALUE_DIM = 128
TOP = 2
ROW_DEV = 256
EXPERTS = 4
CAP = 256
SEQ = 512
ROWS = 1024
N_EP = 4
N_TP = 4


def draw_pair(key):
    base = jax.random.fold_in(key, 17)
    width = HEADS * 2 * HEAD_DIM
    query_key, key_key = jax.random.split(base, 2)
    query_field = jnp.clip(jax.random.normal(query_key, (SEQ, width), jnp.float32) * 1.33, -6.0, 6.0)
    key_field = jnp.clip(jax.random.normal(key_key, (SEQ, width), jnp.float32) * 1.33, -6.0, 6.0)
    return (query_field, key_field)


def draw_queries(key, part):
    return draw_pair(key)[0].astype(jnp.bfloat16)


def draw_keys(key, part):
    return draw_pair(key)[1].astype(jnp.bfloat16)


def block_scale(own_key, extent, pieces, smallest, largest):
    factor_of = 1.0
    for dim, blocks in pieces:
        heights = jax.random.uniform(jax.random.fold_in(jax.random.fold_in(own_key, 6), dim), (blocks,), jnp.float32, smallest / len(pieces), largest / len(pieces))
        factor_of = factor_of * jnp.repeat(jnp.exp(heights), extent[dim] // blocks).reshape((-1,) + (1,) * (len(extent) - 1 - dim))
    return factor_of


def deal_out(own_key, own, number, rows, amount, top, most, slope):
    ranking = jax.random.permutation(own_key, amount)
    heavy_load, usual = shares(amount, rows * top, most, slope, True), shares(amount, rows * top, most, slope, False)
    places = jnp.arange(amount)

    def named(sizes, offset_by):
        used = int((sizes > 0).sum())
        fixed = max(1, used // 4)
        moved = fixed + (places - fixed + offset_by * (used - fixed)) % max(1, amount - fixed)
        return jnp.zeros((amount,), jnp.int32).at[ranking[jnp.where(places < fixed, places, moved)]].set(jnp.asarray(sizes, jnp.int32))

    sizes = jnp.where(number % 4 == 0, named(heavy_load, number // 4), named(usual, number - number // 4 - 1))
    mixed = jax.random.permutation(jax.random.fold_in(own, 3), amount)
    source_of, sink = mixed[0:amount // 2 * 2:2], mixed[1:amount // 2 * 2:2]
    margin = jnp.minimum(sizes[source_of] - 1, most - sizes[sink]) // 2
    margin = jnp.where((source_of == ranking[0]) | (sink == ranking[0]) | (sizes[sink] == 0), 0, jnp.maximum(margin, 0))
    moved = jax.random.randint(jax.random.fold_in(own, 4), (amount // 2,), 0, 1 << 20) % (margin + 1)
    sizes = sizes.at[source_of].add(-moved).at[sink].add(moved)
    items = jnp.searchsorted(jnp.cumsum(sizes), jnp.arange(rows * top), side="right").astype(jnp.int32)
    listing = items.reshape(top, rows).T
    listing = listing[jax.random.permutation(jax.random.fold_in(own, 1), rows)]
    offset_by = jax.random.randint(jax.random.fold_in(own, 2), (rows, 1), 0, top)
    return jnp.take_along_axis(listing, (jnp.arange(top)[None, :] + offset_by) % top, axis=1)


def shares(count, total, bound, slope, full):
    weights = [(1 << 20) // math.isqrt(rank ** slope) + 1 for rank in range(1, count + 1)]
    largest = bound if full else min(bound, max(-(-total // count), total * weights[0] // sum(weights)))
    least = 1 if total - largest >= count - 1 else 0
    counts, surplus = [largest] + [least] * (count - 1), total - largest - least * (count - 1)
    while surplus > 0:
        free = [i for i in range(1, count) if counts[i] < largest] or [i for i in range(1, count) if counts[i] < bound]
        mass, budget = sum([weights[i] for i in free]), surplus
        for i in free:
            more = min(bound - counts[i], max(1, budget * weights[i] // mass), surplus)
            counts[i] = counts[i] + more
            surplus = surplus - more
    return np.array(counts)


def bell_draw(key, dims, spread, limit, shards=(), kind=jnp.bfloat16):
    factor_of = block_scale(key, dims, shards, -0.22, 0.18) if shards else 1.0
    entries = jax.random.normal(key, dims, jnp.float32) * spread * factor_of
    return jnp.minimum(jnp.maximum(entries, -limit), limit).astype(kind)


def setup_inputs(seed: int = 0, part: int = 0) -> dict:
    splits = jax.random.split(jax.random.key(seed), 13)
    own_keys = jax.random.split(jax.random.fold_in(splits[12], part), 13)
    queries = draw_queries(jax.random.fold_in(jax.random.fold_in(splits[12], part), 71), part)
    keys = draw_keys(jax.random.fold_in(jax.random.fold_in(splits[12], part), 71), part)
    values = bell_draw(own_keys[2], (SEQ, HEADS * VALUE_DIM), 1.0, 6.0, ((0, 4), (1, 4)))
    lambdas = jnp.clip(0.3 + 0.5 * jax.random.uniform(splits[3], (HEADS,), jnp.float32) ** block_scale(splits[3], (HEADS,), ((0, 4),), -0.2, 0.2), 0.3, 0.8)
    head_gain = jnp.clip(1.0 + 0.18 * jax.random.normal(splits[4], (VALUE_DIM,), jnp.float32), 0.1, 1.9)
    tokens = bell_draw(own_keys[5], (ROWS, D), 1.0, 6.0, ((0, 4),))
    route_ids_keys = jax.random.split(jax.random.fold_in(own_keys[6], 1), ROWS // ROW_DEV)
    route_ids_turns = jax.random.permutation(jax.random.fold_in(own_keys[6], 3), ROWS // ROW_DEV)
    route_ids = jax.vmap(lambda own, number: deal_out(jax.random.fold_in(own_keys[6], 2), own, number, ROW_DEV, EXPERTS, TOP, CAP, 2))(route_ids_keys, route_ids_turns).reshape((ROWS, TOP))
    route_weights = jnp.clip(0.2 + 0.8 * jax.random.uniform(own_keys[7], (ROWS, TOP), jnp.float32) ** block_scale(own_keys[7], (ROWS, TOP), ((0, 4),), -0.2, 0.2), 0.2, 1.0)
    moe_gain = jnp.clip(1.0 + 0.18 * jax.random.normal(splits[8], (D,), jnp.float32), 0.1, 1.9)
    w_gate = bell_draw(splits[9], (EXPERTS, D, FF), D ** -0.5, 0.15625, ((0, 4), (2, 4)))
    w_up = bell_draw(splits[10], (EXPERTS, D, FF), D ** -0.5, 0.15625, ((0, 4), (2, 4)))
    w_down = bell_draw(splits[11], (EXPERTS, FF, D), FF ** -0.5, 0.109375, ((0, 4), (1, 4)))
    return dict(queries=queries, keys=keys, values=values, lambdas=lambdas, head_gain=head_gain, tokens=tokens, route_ids=route_ids, route_weights=route_weights, moe_gain=moe_gain, w_gate=w_gate, w_up=w_up, w_down=w_down)


def head_mix(operands):
    query_head, key_head, value_head, lambda_head, head_gain = operands
    block = math.gcd(SEQ, 512)
    query_blocks = query_head.reshape(SEQ // block, block, 2, HEAD_DIM)

    def one_block(query_part):
        results = []
        for component in range(2):
            scores = jnp.dot(query_part[:, component], key_head[:, component].T, preferred_element_type=jnp.float32) * HEAD_DIM ** (-0.5)
            highest = lax.optimization_barrier(jnp.max(scores, axis=1, keepdims=True))
            shifted = jnp.exp(scores - highest)
            totals = lax.optimization_barrier(jnp.sum(shifted, axis=1, keepdims=True))
            sums = jnp.dot(shifted.astype(jnp.bfloat16), value_head, preferred_element_type=jnp.float32)
            results.append(sums / totals)
        mixed = results[0] - lambda_head * results[1]
        scaled = mixed * lax.rsqrt(lax.optimization_barrier(jnp.mean(mixed * mixed, axis=1, keepdims=True)) + 1e-06) * head_gain
        return scaled.astype(jnp.bfloat16)
    return lax.map(one_block, query_blocks).reshape(SEQ, VALUE_DIM)

def reference(queries, keys, values, lambdas, head_gain, tokens, route_ids, route_weights, moe_gain, w_gate, w_up, w_down):
    query_heads = jnp.transpose(queries.reshape(SEQ, HEADS, 2, HEAD_DIM), (1, 0, 2, 3))
    key_heads = jnp.transpose(keys.reshape(SEQ, HEADS, 2, HEAD_DIM), (1, 0, 2, 3))
    value_heads = jnp.transpose(values.reshape(SEQ, HEADS, VALUE_DIM), (1, 0, 2))
    gains = jnp.broadcast_to(head_gain, (HEADS, VALUE_DIM))
    mixed_heads = lax.map(head_mix, (query_heads, key_heads, value_heads, lambdas, gains))
    heads_out = jnp.transpose(mixed_heads, (1, 0, 2)).reshape(SEQ, HEADS * VALUE_DIM)
    token_float = tokens.astype(jnp.float32)
    normed = (token_float * lax.rsqrt(lax.optimization_barrier(jnp.mean(token_float * token_float, axis=1, keepdims=True)) + 1e-06) * moe_gain).astype(jnp.bfloat16)
    flat_ids = route_ids.reshape(N_EP, ROW_DEV * TOP)
    onehot = (flat_ids[:, :, None] == jnp.arange(EXPERTS, dtype=jnp.int32)[None, None, :]).astype(jnp.int32)
    earlier = jnp.cumsum(onehot, axis=1) - onehot
    position = lax.optimization_barrier(jnp.sum(earlier * onehot, axis=2)).astype(jnp.int32)
    source = jnp.broadcast_to(jnp.arange(N_EP, dtype=jnp.int32)[:, None], (N_EP, ROW_DEV * TOP))
    owner_row = source * ROW_DEV + jnp.arange(ROW_DEV * TOP, dtype=jnp.int32)[None, :] // TOP
    table = jnp.full((EXPERTS, N_EP, CAP), ROWS, jnp.int32).at[flat_ids, source, position].set(owner_row)
    padded = jnp.concatenate([normed, jnp.zeros((1, D), jnp.bfloat16)], axis=0)

    def expert_pass(operands):
        rows_index, gate_mat, up_mat, down_mat = operands
        arrived = padded[rows_index.reshape(-1)]
        gate = jnp.dot(arrived, gate_mat, preferred_element_type=jnp.float32)
        upward = jnp.dot(arrived, up_mat, preferred_element_type=jnp.float32)
        hidden = (jax.nn.silu(gate) * upward).astype(jnp.bfloat16)
        hidden_blocks = jnp.transpose(hidden.reshape(-1, N_TP, FF // N_TP), (1, 0, 2)).astype(jnp.float32)
        down_blocks = down_mat.reshape(N_TP, FF // N_TP, D).astype(jnp.float32)
        partial_sums = jnp.einsum('jsf,jfd->jsd', hidden_blocks, down_blocks)
        rounded = lax.optimization_barrier(partial_sums.astype(jnp.bfloat16))
        return lax.optimization_barrier(jnp.sum(rounded.astype(jnp.float32), axis=0)).astype(jnp.bfloat16)
    results = lax.map(expert_pass, (table, w_gate, w_up, w_down)).reshape(EXPERTS, N_EP, CAP, D)
    picked = results[flat_ids, source, position].reshape(ROWS, TOP, D).astype(jnp.float32)
    expert_out = jnp.einsum('rkd,rk->rd', picked, route_weights).astype(jnp.bfloat16)
    return (heads_out, expert_out)
```

```python
import functools

import jax
import jax.numpy as jnp
from jax import lax
from jax.experimental import pallas as pl
from jax.experimental.pallas import tpu as pltpu
from jax.sharding import PartitionSpec as P

MESH = pl.DeviceIdType.MESH
F32 = jnp.float32
BF16 = jnp.bfloat16
PIECES = 4
OUTER_VISIT = 2

def attend(queries, keys, values, lambdas, head_gain):
    row_count = queries.shape[0]
    head_count = lambdas.shape[0]
    head_dim = queries.shape[1] // (2 * head_count)
    value_dim = values.shape[1] // head_count
    query_parts = queries.reshape(row_count, head_count, 2, head_dim)
    score_scale = head_dim ** (-0.5)
    running = jnp.full((head_count, 2, row_count), -1e30, jnp.float32)
    key_piece = lax.all_gather(keys, "ep", axis=0, tiled=True)
    value_piece = lax.all_gather(values, "ep", axis=0, tiled=True)
    count = key_piece.shape[0]
    key_parts = key_piece.reshape(count, head_count, 2, head_dim)
    value_parts = value_piece.reshape(count, head_count, value_dim)
    scores = (
        jnp.einsum("qhcd,khcd->hcqk", query_parts, key_parts, preferred_element_type=jnp.float32)
        * score_scale
    )
    newest = jnp.maximum(running, jnp.max(scores, axis=-1))
    weights_now = jnp.exp(scores - newest[..., None])
    totals = jnp.sum(weights_now, axis=-1)
    sums = jnp.einsum(
        "hcqk,khe->hcqe",
        weights_now.astype(jnp.bfloat16),
        value_parts,
        preferred_element_type=jnp.float32,
    )
    running, totals, sums = (newest, totals, sums)
    means = sums / totals[..., None]
    mixed = means[:, 0] - lambdas[:, None, None] * means[:, 1]
    scaled = mixed * lax.rsqrt(jnp.mean(mixed * mixed, axis=-1, keepdims=True) + 1e-06) * head_gain
    return (
        jnp.transpose(scaled, (1, 0, 2))
        .reshape(row_count, head_count * value_dim)
        .astype(jnp.bfloat16)
    )


def experts(tokens, route_ids, route_weights, moe_gain, w_gate, w_up, w_down):
    row_count, width = tokens.shape
    top_count = route_ids.shape[1]
    ep_size = lax.axis_size("ep")
    tp_size = lax.axis_size("tp")
    expert_count = w_gate.shape[0] * ep_size
    capacity = 2 * row_count * top_count // expert_count
    token_float = tokens.astype(jnp.float32)
    normed = (
        token_float
        * lax.rsqrt(jnp.mean(token_float * token_float, axis=1, keepdims=True) + 1e-06)
        * moe_gain
    ).astype(jnp.bfloat16)
    flat_ids = route_ids.reshape(-1)
    onehot = (flat_ids[:, None] == jnp.arange(expert_count, dtype=jnp.int32)[None, :]).astype(
        jnp.int32
    )
    earlier = jnp.cumsum(onehot, axis=0) - onehot
    position = jnp.sum(earlier * onehot, axis=1)
    slot_index = flat_ids * capacity + position
    owners = (
        jnp.full((expert_count * capacity,), row_count, jnp.int32)
        .at[slot_index]
        .set(jnp.arange(row_count * top_count, dtype=jnp.int32) // top_count)
    )
    padded = jnp.concatenate([normed, jnp.zeros((1, width), jnp.bfloat16)], axis=0)
    outgoing = padded[owners].reshape(expert_count, capacity, width)
    gate_mat = w_gate[0]
    up_mat = w_up[0]
    down_mat = w_down[0]
    slice_width = width // tp_size
    own_columns = lax.dynamic_slice_in_dim(
        outgoing, lax.axis_index("tp") * slice_width, slice_width, 2
    )
    arrived = lax.all_to_all(own_columns, "ep", split_axis=0, concat_axis=0, tiled=True)
    piece = lax.all_gather(arrived, "tp", axis=2, tiled=True)
    gate = jnp.einsum("scd,df->scf", piece, gate_mat, preferred_element_type=jnp.float32)
    upward = jnp.einsum("scd,df->scf", piece, up_mat, preferred_element_type=jnp.float32)
    hidden = (jax.nn.silu(gate) * upward).astype(jnp.bfloat16)
    flat_hidden = hidden.reshape(-1, hidden.shape[2])
    summed = lax.psum_scatter(
        jnp.einsum("fd,sf->ds", down_mat, flat_hidden, preferred_element_type=jnp.float32).astype(
            jnp.bfloat16
        ),
        "tp",
        scatter_dimension=0,
        tiled=True,
    )
    back = lax.all_to_all(summed, "ep", split_axis=1, concat_axis=1, tiled=True)
    picked = (
        jnp.take(back, slot_index, axis=1).astype(jnp.float32).reshape(-1, row_count, top_count)
    )
    combined = jnp.einsum("drk,rk->rd", picked, route_weights)
    return combined.astype(jnp.bfloat16)


def visit_order(n):
    def key(e):
        left = 2 * e < n
        outward = (lambda s: s < e) if left else (lambda s: s > e)
        return lambda s: (outward(s), abs(s - e))

    return [sorted((s for s in range(n) if s != e), key=key(e)) for e in range(n)]


def fused_kernel(
    n,
    q_hbm,
    k_hbm,
    v_hbm,
    lam_hbm,
    hgain_hbm,
    tok_hbm,
    ids_hbm,
    rw_hbm,
    mgain_hbm,
    wg_hbm,
    wu_hbm,
    wd_hbm,
    heads_ref,
    out_ref,
    wg,
    wu,
    wd,
    q_ref,
    lam_ref,
    hgain_ref,
    tok_ref,
    ids_ref,
    rw_ref,
    mgain_ref,
    gathered,
    kv,
    hid,
    part,
    core_in,
    s_own,
    s_out,
    x_in,
    t_out,
    ret,
    z_out,
    z_in,
    out_weights,
    wsem,
    tok_sem,
    in_sem,
    own_send,
    z_send,
    z_recv,
    x_send,
    x_recv,
    c_send,
    c_recv,
    kv_own_send,
    kv_send,
    kv_recv,
    r1_send,
    r1_recv,
    r2_send,
    r2_recv,
    r3_send,
    r3_recv,
    zo_send,
    zo_recv,
):
    e = lax.axis_index("ep")
    t = lax.axis_index("tp")
    xi = t // 2
    ci = lax.rem(t, 2)
    core_peer = {"tp": 2 * xi + 1 - ci}
    tx = 2 * (1 - xi) + ci
    x_peer = {"tp": tx}
    rows, width = tok_ref.shape
    cols = width // 4
    kv_rows = k_hbm.shape[0]
    has_left = e > 0
    has_right = e < n - 1
    inner = jnp.logical_and(has_left, has_right)
    outer = jnp.logical_not(inner)
    left_half = 2 * e < n
    inward = {"ep": jnp.clip(jnp.where(left_half, e + 1, e - 1), 0, n - 1)}
    outward = {"ep": jnp.clip(jnp.where(left_half, e - 1, e + 1), 0, n - 1)}

    def colblock(j):
        return pl.ds(pl.multiple_of(j * cols, 128), cols)

    def remote(src, dst, ss, rs, dev):
        return pltpu.make_async_remote_copy(
            src_ref=src, dst_ref=dst, send_sem=ss, recv_sem=rs, device_id=dev, device_id_type=MESH
        )

    barrier = pltpu.get_barrier_semaphore()
    pl.semaphore_signal(barrier, inc=1, device_id=inward, device_id_type=MESH)

    @pl.when(inner)
    def _():
        pl.semaphore_signal(barrier, inc=1, device_id=outward, device_id_type=MESH)

    pl.semaphore_signal(barrier, inc=1, device_id=core_peer, device_id_type=MESH)
    pl.semaphore_signal(barrier, inc=1, device_id=x_peer, device_id_type=MESH)
    greeted = 3 + inner.astype(jnp.int32)

    halves = range(PIECES)
    early, late = halves[: PIECES // 2], halves[PIECES // 2 :]
    hr = rows // PIECES

    def half(h):
        return pl.ds(h * hr, hr)

    own_kv = pl.ds(pl.multiple_of(e * kv_rows, kv_rows), kv_rows)
    k_width = k_hbm.shape[1]
    v_width = v_hbm.shape[1]
    gain_in = pltpu.make_async_copy(mgain_hbm, mgain_ref, in_sem.at[0])
    gain_in.start()
    tokens_in = pltpu.make_async_copy(tok_hbm, tok_ref, tok_sem.at[0])
    tokens_in.start()
    weights = [
        pltpu.make_async_copy(a, b, wsem.at[i])
        for i, (a, b) in enumerate(((wg_hbm.at[0], wg), (wu_hbm.at[0], wu), (wd_hbm.at[0], wd)))
    ]
    kv_in = [
        pltpu.make_async_copy(k_hbm, kv.at[own_kv, pl.ds(0, k_width)], in_sem.at[1]),
        pltpu.make_async_copy(v_hbm, kv.at[own_kv, pl.ds(k_width, v_width)], in_sem.at[2]),
    ]
    others_in = [
        pltpu.make_async_copy(a, b, in_sem.at[i + 3])
        for i, (a, b) in enumerate(
            ((ids_hbm, ids_ref), (rw_hbm, rw_ref), (q_hbm, q_ref), (lam_hbm, lam_ref), (hgain_hbm, hgain_ref))
        )
    ]

    def normalize(h):
        step = 32

        @pl.loop(0, hr // step)
        def _(i):
            sl = pl.ds(pl.multiple_of(h * hr + i * step, step), step)
            v = tok_ref[sl, :].astype(F32)
            scale = lax.rsqrt(jnp.mean(v * v, axis=1, keepdims=True) + 1e-06)
            gathered[e, sl, :] = (v * scale * mgain_ref[...]).astype(BF16)

    def own_tok(side, h):
        blk = gathered.at[e, half(h), colblock(t)]
        return remote(blk, blk, own_send.at[0], z_recv.at[e, h], (inward, outward)[side])

    def own_tok2(h):
        blk = gathered.at[e, half(h), colblock(tx)]
        return remote(blk, blk, own_send.at[0], x_recv.at[e, h], inward)

    def own_kv_copy(side):
        blk = kv.at[own_kv]
        return remote(blk, blk, kv_own_send.at[0], kv_recv.at[e], (inward, outward)[side])

    orders = visit_order(n)

    def nth(k):
        s = jnp.int32(orders[0][k])
        for i in range(1, n):
            s = jnp.where(e == i, jnp.int32(orders[i][k]), s)
        return s

    visits = [nth(k) for k in range(n - 1)]

    def onward(k):
        return inward if k == OUTER_VISIT else outward

    def z_copy(k, h):
        blk = gathered.at[visits[k], half(h), colblock(t)]
        return remote(blk, blk, z_send.at[0], z_recv.at[visits[k], h], onward(k))

    def kv_copy(k):
        s = visits[k]
        blk = kv.at[pl.ds(pl.multiple_of(s * kv_rows, kv_rows), kv_rows)]
        return remote(blk, blk, kv_send.at[0], kv_recv.at[s], onward(k))

    def x_copy(s, h):
        blk = gathered.at[s, half(h), colblock(t)]
        return remote(blk, blk, x_send.at[0], x_recv.at[s, h], x_peer)

    def c_copy(s, h, which):
        blk = gathered.at[s, half(h), colblock((t, tx)[which])]
        return remote(blk, blk, c_send.at[0], c_recv.at[s], core_peer)

    def r1_copy(s, xx):
        return remote(
            part.at[s, :, colblock(2 * xx + 1 - ci)],
            core_in.at[s, xx],
            r1_send.at[0],
            r1_recv.at[xx, s],
            core_peer,
        )

    def r2_copy(s, h):
        return remote(
            s_out.at[s, half(h)], x_in.at[s, half(h)], r2_send.at[s], r2_recv.at[s, h], x_peer
        )

    def r3_copy(s, h):
        return remote(
            t_out.at[s, half(h)],
            ret.at[e, half(h)],
            r3_send.at[0],
            r3_recv.at[e, h],
            {"ep": s},
        )

    def r3_back(s, h):
        return remote(
            t_out.at[s, half(h)],
            ret.at[s, half(h)],
            r3_send.at[0],
            r3_recv.at[s, h],
            {"ep": s},
        )

    def zo_copy(i, h):
        return remote(
            z_out.at[i, half(h)], z_in.at[i, half(h)], zo_send.at[0], zo_recv.at[i, h], inward
        )

    ff = wg.shape[1]
    nb = ff // 3

    def up_step(s, b):
        sl = pl.ds(b * nb, nb)
        g = jnp.dot(gathered[s], wg[:, sl], preferred_element_type=F32)
        u = jnp.dot(gathered[s], wu[:, sl], preferred_element_type=F32)
        hid[:, sl] = (g / (1.0 + jnp.exp(-g)) * u).astype(BF16)

    def down_step(s, j):
        sl = colblock(j)
        part[s, :, sl] = jnp.dot(hid[...], wd[:, sl], preferred_element_type=F32).astype(BF16)

    def down_far(s):
        down_step(s, 2 * (1 - xi) + 1 - ci)
        r1_copy(s, 1 - xi).start()
        down_step(s, tx)

    def down_near(s):
        down_step(s, 2 * xi + 1 - ci)
        r1_copy(s, xi).start()
        down_step(s, t)

    def across(s, h):
        return part[s, half(h), colblock(tx)].astype(F32) + core_in[s, 1 - xi, half(h)].astype(F32)

    def along(s, h):
        return part[s, half(h), colblock(t)].astype(F32) + core_in[s, xi, half(h)].astype(F32)

    def reduce_core(s):
        r1_copy(s, 1 - xi).wait_recv()
        for h in halves:
            s_out[s, half(h)] = across(s, h).astype(BF16)
            r2_copy(s, h).start()

    def reduce_z(s):
        r1_copy(s, 1 - xi).wait_recv()
        for h in halves:
            z_out[0, half(h)] = across(s, h).astype(BF16)
            zo_copy(0, h).start()
        r1_copy(s, xi).wait_recv()
        for h in halves:
            z_out[1, half(h)] = along(s, h).astype(BF16)
            zo_copy(1, h).start()

    def own_sums():
        r1_copy(e, 1 - xi).wait_recv()
        r1_copy(e, xi).wait_recv()

    def reduce_own(h, joined):
        w = out_weights[half(h), 0:1]
        there = across(e, h) * w
        here = along(e, h) * w
        if joined:
            zo_copy(0, h).wait_recv()
            zo_copy(1, h).wait_recv()
            v = out_weights[half(h), OUTER_VISIT + 1 : OUTER_VISIT + 2]
            there = there + z_in[0, half(h)].astype(F32) * v
            here = here + z_in[1, half(h)].astype(F32) * v
        s_out[e, half(h)] = there.astype(BF16)
        r2_copy(e, h).start()
        s_own[half(h)] = here

    def reduce_x(s, h):
        if h == 0:
            r1_copy(s, xi).wait_recv()
        r2_copy(s, h).wait_recv()
        t_out[s, half(h)] = (along(s, h) + x_in[s, half(h)].astype(F32)).astype(BF16)
        r3_copy(s, h).start()

    def arrive(k, h, x=True):
        z_copy(k, h).wait_recv()
        if x:
            x_copy(visits[k], h).start()
        c_copy(visits[k], h, 0).start()

    def relay(k, h, x=True):
        z_copy(k, h).wait_recv()
        z_copy(k, h).start()
        if x:
            x_copy(visits[k], h).start()
        c_copy(visits[k], h, 0).start()

    def cross(k, h):
        x_copy(visits[k], h).wait_recv()
        c_copy(visits[k], h, 1).start()

    def waiter(ref, ss, rs):
        return remote(ref, ref, ss, rs, core_peer)

    def ready(s):
        waiter(gathered.at[s, :, pl.ds(0, 2 * cols)], c_send.at[0], c_recv.at[s]).wait_recv()

    def attend(h):
        heads = lam_ref.shape[0]
        vd = v_width // heads
        hd = q_ref.shape[1] // (2 * heads)
        qr = q_ref.shape[0]
        first = lax.broadcasted_iota(jnp.int32, (qr, 2 * hd), 1) < hd
        q = q_ref[:, h * 2 * hd : (h + 1) * 2 * hd].astype(F32)
        both = jnp.concatenate(
            [jnp.where(first, q, 0.0).astype(BF16), jnp.where(first, 0.0, q).astype(BF16)], axis=0
        )
        kh = kv[:, h * 2 * hd : (h + 1) * 2 * hd]
        vh = kv[:, k_width + h * vd : k_width + (h + 1) * vd]
        scores = lax.dot_general(
            both, kh, (((1,), (1,)), ((), ())), preferred_element_type=F32
        ) * (hd ** (-0.5))
        ex = jnp.exp(scores - jnp.max(scores, axis=1, keepdims=True))
        tot = jnp.sum(ex, axis=1, keepdims=True)
        sums = jnp.dot(ex.astype(BF16), vh, preferred_element_type=F32) / tot
        mixed = sums[:qr] - lam_ref[h] * sums[qr:]
        norm = lax.rsqrt(jnp.mean(mixed * mixed, axis=1, keepdims=True) + 1e-06)
        heads_ref[:, h * vd : (h + 1) * vd] = (mixed * norm * hgain_ref[...]).astype(BF16)

    def add_back(k, h, end):
        r3_back(visits[k], h).wait_recv()
        w = out_weights[half(h), k + 1 : k + 2]
        total = s_own[half(h)] + ret[visits[k], half(h)].astype(F32) * w
        if end:
            out_ref[half(h), :] = total.astype(BF16)
        else:
            s_own[half(h)] = total

    def on_inner(fn):
        pl.when(inner)(fn)

    def on_outer(fn):
        pl.when(outer)(fn)

    def at(out, inn):
        if out:

            @on_outer
            def _():
                for f, *args in out:
                    f(*args)

        if inn:

            @on_inner
            def _():
                for f, *args in inn:
                    f(*args)

    def start_kv(side):
        own_kv_copy(side).start()

    def take_kv(k):
        kv_copy(k).wait_recv()

    def pass_kv(k):
        kv_copy(k).wait_recv()
        kv_copy(k).start()

    def start_tok2(h):
        own_tok2(h).start()

    def relays(h):
        relay(2, h, False)
        relay(0, h)

    gain_in.wait()
    for c in kv_in + others_in:
        c.start()
    tokens_in.wait()
    for c in weights:
        c.start()
    for h in halves:
        normalize(h)
        if h == 0:
            pl.semaphore_wait(barrier, greeted)
        own_tok(0, h).start()

        @on_inner
        def _():
            own_tok(1, h).start()

    for c in kv_in + others_in:
        c.wait()
    ids = ids_ref[...]
    rw = rw_ref[...]
    lines = [jnp.sum(jnp.where(ids == x, rw, 0.0), axis=0, keepdims=True) for x in [e] + visits]
    pad = (-len(lines)) % 8
    lines.append(jnp.zeros((pad, rows), F32))
    out_weights[...] = jnp.concatenate(lines, axis=0).T

    for c in weights:
        c.wait()
    v0, v1, v2 = visits
    up_step(e, 0)
    at([(arrive, 0, 0), (start_tok2, 0)], [(relays, 0)])
    up_step(e, 1)
    at([(arrive, 0, 1), (start_tok2, 1)], [(relays, 1)])
    up_step(e, 2)
    at([(arrive, 0, 2), (start_tok2, 2)], [(relays, 2)])
    down_far(e)
    at(
        [(start_tok2, 3), (arrive, 0, 3), (start_kv, 0), (cross, 0, 0)],
        [(relays, 3), (cross, 0, 0)],
    )
    down_near(e)
    at(
        [
            (arrive, 1, 0), (cross, 0, 1), (arrive, 1, 1), (cross, 0, 2), (arrive, 1, 2),
            (cross, 0, 3),
        ],
        [
            (relay, 1, 0), (cross, 0, 1), (cross, 2, 0), (relay, 1, 1), (cross, 0, 2), (cross, 2, 1),
            (relay, 1, 2), (cross, 0, 3), (cross, 2, 2), (start_kv, 0),
        ],
    )
    ready(v0)
    up_step(v0, 0)
    at([(arrive, 1, 3), (cross, 1, 0)], [(relay, 1, 3), (cross, 2, 3), (start_kv, 1), (cross, 1, 0)])
    up_step(v0, 1)
    at([(arrive, 2, 0), (cross, 1, 1)], [(cross, 1, 1)])
    up_step(v0, 2)
    at([(arrive, 2, 1), (cross, 1, 2)], [(cross, 1, 2)])
    down_far(v0)
    at([(arrive, 2, 2), (cross, 1, 3)], [(cross, 1, 3)])
    down_near(v0)
    own_sums()
    at([(arrive, 2, 3)] + [(reduce_own, h, False) for h in early], [(reduce_core, v0)])
    ready(v1)
    up_step(v1, 0)
    at([(reduce_z, v0), (cross, 2, 0), (cross, 2, 1)], [(pass_kv, 2)])
    up_step(v1, 1)
    at([(cross, 2, 2)], [])
    up_step(v1, 2)
    down_far(v1)
    at([(cross, 2, 3)], [(pass_kv, 0)])
    down_near(v1)
    reduce_core(v1)
    at([], [(reduce_x, v0, h) for h in early])
    ready(v2)
    up_step(v2, 0)
    at([], [(reduce_x, v0, 2)])
    up_step(v2, 1)
    at([], [(pass_kv, 1)])
    up_step(v2, 2)
    at([], [(reduce_x, v0, 3)])
    down_far(v2)
    at([(reduce_x, v1, 0)], [])
    down_near(v2)
    reduce_core(v2)
    reduce_rest = [(reduce_x, v1, h) for h in early]
    at(reduce_rest[1:], reduce_rest)
    at([(take_kv, k) for k in range(n - 1)], [])
    attend(0)
    reduce_x(v1, 2)
    for h in range(1, lam_ref.shape[0]):
        attend(h)
    reduce_x(v1, 3)

    def settle(joined, hs):
        waiter(s_out.at[v2], r2_send.at[v2], r2_recv.at[v2, 0]).wait_send()
        for h in hs:
            reduce_own(h, joined)
        for h in halves:
            reduce_x(v2, h)

    at([(settle, False, late)], [(settle, True, halves)])

    for h in halves:
        r2_copy(e, h).wait_recv()
        s_own[half(h)] = s_own[half(h)] + x_in[e, half(h)].astype(F32)

    def gather_back(ks):
        for k in ks:
            for h in halves:
                add_back(k, h, k == ks[-1])

    @on_outer
    def _():
        gather_back((1, 0, 2))

    @on_inner
    def _():
        gather_back((0, 1))

    def sent(ref, sem):
        waiter(ref, sem, c_recv.at[e]).wait_send()

    quarter, double = pl.ds(0, cols), pl.ds(0, 2 * cols)
    sent(part.at[:, :, double], r1_send.at[0])
    sent(gathered.at[pl.ds(0, 3), :, double], c_send.at[0])
    sent(gathered.at[pl.ds(0, 2), :, quarter], own_send.at[0])
    sent(s_out.at[e], r2_send.at[e])
    sent(s_out.at[v1], r2_send.at[v1])

    @on_outer
    def _():
        sent(kv.at[pl.ds(0, kv_rows)], kv_own_send.at[0])
        sent(gathered.at[pl.ds(0, 3), :, quarter], x_send.at[0])
        sent(z_out, zo_send.at[0])
        sent(t_out.at[pl.ds(0, 2)], r3_send.at[0])

    @on_inner
    def _():
        sent(kv.at[pl.ds(0, 2 * kv_rows)], kv_own_send.at[0])
        sent(kv.at[pl.ds(0, 3 * kv_rows)], kv_send.at[0])
        sent(gathered.at[pl.ds(0, 3), :, quarter], z_send.at[0])
        sent(gathered.at[pl.ds(0, 2), :, quarter], x_send.at[0])
        sent(s_out.at[v0], r2_send.at[v0])
        sent(t_out.at[pl.ds(0, 3)], r3_send.at[0])


def hand_on_kernel(a_ref, b_ref, c_ref, d_ref):
    c_ref[...] = a_ref[...]
    d_ref[...] = b_ref[...]


def fused(queries, keys, values, lambdas, head_gain, tokens, route_ids, route_weights, moe_gain, w_gate, w_up, w_down):
    n = lax.axis_size("ep")
    rows, width = tokens.shape
    cols = width // 4
    ff = w_gate.shape[2]
    vmem = pl.BlockSpec(memory_space=pltpu.VMEM)
    hbm = pl.BlockSpec(memory_space=pltpu.HBM)
    dma = pltpu.SemaphoreType.DMA
    results = pl.pallas_call(
        functools.partial(fused_kernel, n),
        out_shape=(
            pltpu.VMEM((queries.shape[0], values.shape[1]), BF16),
            pltpu.VMEM((rows, cols), BF16),
        ),
        in_specs=[hbm] * 12,
        out_specs=(vmem, vmem),
        scratch_shapes=[
            pltpu.VMEM((width, ff), BF16),
            pltpu.VMEM((width, ff), BF16),
            pltpu.VMEM((ff, width), BF16),
            pltpu.VMEM(queries.shape, BF16),
            pltpu.SMEM(lambdas.shape, F32),
            pltpu.VMEM(head_gain.shape, F32),
            pltpu.VMEM((rows, width), BF16),
            pltpu.VMEM(route_ids.shape[::-1], jnp.int32),
            pltpu.VMEM(route_weights.shape[::-1], F32),
            pltpu.VMEM(moe_gain.shape, F32),
            pltpu.VMEM((n, rows, width), BF16),
            pltpu.VMEM((n * keys.shape[0], keys.shape[1] + values.shape[1]), BF16),
            pltpu.VMEM((rows, ff), BF16),
            pltpu.VMEM((n, rows, width), BF16),
            pltpu.VMEM((n, 2, rows, cols), BF16),
            pltpu.VMEM((rows, cols), F32),
            pltpu.VMEM((n, rows, cols), BF16),
            pltpu.VMEM((n, rows, cols), BF16),
            pltpu.VMEM((n, rows, cols), BF16),
            pltpu.VMEM((n, rows, cols), BF16),
            pltpu.VMEM((2, rows, cols), BF16),
            pltpu.VMEM((2, rows, cols), BF16),
            pltpu.VMEM((rows, -(-n // 8) * 8), F32),
            dma((3,)),
            dma((1,)),
            dma((8,)),
            dma((1,)),
            dma((1,)),
            dma((n, PIECES)),
            dma((1,)),
            dma((n, PIECES)),
            dma((1,)),
            dma((n,)),
            dma((1,)),
            dma((1,)),
            dma((n,)),
            dma((1,)),
            dma((2, n)),
            dma((n,)),
            dma((n, PIECES)),
            dma((1,)),
            dma((n, PIECES)),
            dma((1,)),
            dma((2, PIECES)),
        ],
        compiler_params=pltpu.CompilerParams(
            collective_id=0, has_side_effects=True, vmem_limit_bytes=60 * 1024 * 1024
        ),
        name="fused_layer",
    )(
        queries,
        keys,
        values,
        lambdas,
        head_gain,
        tokens,
        route_ids.T,
        route_weights.T,
        moe_gain,
        w_gate,
        w_up,
        w_down,
    )
    return pl.pallas_call(
        hand_on_kernel,
        out_shape=tuple(jax.ShapeDtypeStruct(r.shape, r.dtype) for r in results),
        in_specs=[vmem, vmem],
        out_specs=(vmem, vmem),
        compiler_params=pltpu.CompilerParams(vmem_limit_bytes=4 * 1024 * 1024),
        name="hand_on",
    )(*results)


def on_device(
    queries,
    keys,
    values,
    lambdas,
    head_gain,
    tokens,
    route_ids,
    route_weights,
    moe_gain,
    w_gate,
    w_up,
    w_down,
):
    rows = tokens.shape[0]
    expert_count = w_gate.shape[0] * lax.axis_size("ep")
    slots = 2 * rows * route_ids.shape[1] // expert_count
    if w_gate.shape[0] == 1 and lax.axis_size("tp") == lax.axis_size("ep") == 4 and slots >= rows:
        return fused(
            queries, keys, values, lambdas, head_gain, tokens,
            route_ids, route_weights, moe_gain, w_gate, w_up, w_down,
        )
    heads_out = attend(queries, keys, values, lambdas, head_gain)
    expert_out = experts(tokens, route_ids, route_weights, moe_gain, w_gate, w_up, w_down)
    return (heads_out, expert_out)


def solution(mesh):
    in_specs = (
        P(("grp", "ep"), "tp"),
        P(("grp", "ep"), "tp"),
        P(("grp", "ep"), "tp"),
        P("tp"),
        P(),
        P(("grp", "ep"), None),
        P(("grp", "ep"), None),
        P(("grp", "ep"), None),
        P(),
        P("ep", None, "tp"),
        P("ep", None, "tp"),
        P("ep", "tp", None),
    )
    out_specs = (P(("grp", "ep"), "tp"), P(("grp", "ep"), "tp"))
    return jax.shard_map(
        on_device, mesh=mesh, in_specs=in_specs, out_specs=out_specs, check_vma=False
    )
```

```python
import functools

import jax
import jax.numpy as jnp
from jax import lax
from jax.experimental import pallas as pl
from jax.experimental.pallas import tpu as pltpu
from jax.sharding import PartitionSpec as P

MESH = pl.DeviceIdType.MESH
F32 = jnp.float32
BF16 = jnp.bfloat16
PIECES = 4
OUTER_VISIT = 0

def attend(queries, keys, values, lambdas, head_gain):
    row_count = queries.shape[0]
    head_count = lambdas.shape[0]
    head_dim = queries.shape[1] // (2 * head_count)
    value_dim = values.shape[1] // head_count
    query_parts = queries.reshape(row_count, head_count, 2, head_dim)
    score_scale = head_dim ** (-0.5)
    running = jnp.full((head_count, 2, row_count), -1e30, jnp.float32)
    key_piece = lax.all_gather(keys, "ep", axis=0, tiled=True)
    value_piece = lax.all_gather(values, "ep", axis=0, tiled=True)
    count = key_piece.shape[0]
    key_parts = key_piece.reshape(count, head_count, 2, head_dim)
    value_parts = value_piece.reshape(count, head_count, value_dim)
    scores = (
        jnp.einsum("qhcd,khcd->hcqk", query_parts, key_parts, preferred_element_type=jnp.float32)
        * score_scale
    )
    newest = jnp.maximum(running, jnp.max(scores, axis=-1))
    weights_now = jnp.exp(scores - newest[..., None])
    totals = jnp.sum(weights_now, axis=-1)
    sums = jnp.einsum(
        "hcqk,khe->hcqe",
        weights_now.astype(jnp.bfloat16),
        value_parts,
        preferred_element_type=jnp.float32,
    )
    running, totals, sums = (newest, totals, sums)
    means = sums / totals[..., None]
    mixed = means[:, 0] - lambdas[:, None, None] * means[:, 1]
    scaled = mixed * lax.rsqrt(jnp.mean(mixed * mixed, axis=-1, keepdims=True) + 1e-06) * head_gain
    return (
        jnp.transpose(scaled, (1, 0, 2))
        .reshape(row_count, head_count * value_dim)
        .astype(jnp.bfloat16)
    )


def experts(tokens, route_ids, route_weights, moe_gain, w_gate, w_up, w_down):
    row_count, width = tokens.shape
    top_count = route_ids.shape[1]
    ep_size = lax.axis_size("ep")
    tp_size = lax.axis_size("tp")
    expert_count = w_gate.shape[0] * ep_size
    capacity = 2 * row_count * top_count // expert_count
    token_float = tokens.astype(jnp.float32)
    normed = (
        token_float
        * lax.rsqrt(jnp.mean(token_float * token_float, axis=1, keepdims=True) + 1e-06)
        * moe_gain
    ).astype(jnp.bfloat16)
    flat_ids = route_ids.reshape(-1)
    onehot = (flat_ids[:, None] == jnp.arange(expert_count, dtype=jnp.int32)[None, :]).astype(
        jnp.int32
    )
    earlier = jnp.cumsum(onehot, axis=0) - onehot
    position = jnp.sum(earlier * onehot, axis=1)
    slot_index = flat_ids * capacity + position
    owners = (
        jnp.full((expert_count * capacity,), row_count, jnp.int32)
        .at[slot_index]
        .set(jnp.arange(row_count * top_count, dtype=jnp.int32) // top_count)
    )
    padded = jnp.concatenate([normed, jnp.zeros((1, width), jnp.bfloat16)], axis=0)
    outgoing = padded[owners].reshape(expert_count, capacity, width)
    gate_mat = w_gate[0]
    up_mat = w_up[0]
    down_mat = w_down[0]
    slice_width = width // tp_size
    own_columns = lax.dynamic_slice_in_dim(
        outgoing, lax.axis_index("tp") * slice_width, slice_width, 2
    )
    arrived = lax.all_to_all(own_columns, "ep", split_axis=0, concat_axis=0, tiled=True)
    piece = lax.all_gather(arrived, "tp", axis=2, tiled=True)
    gate = jnp.einsum("scd,df->scf", piece, gate_mat, preferred_element_type=jnp.float32)
    upward = jnp.einsum("scd,df->scf", piece, up_mat, preferred_element_type=jnp.float32)
    hidden = (jax.nn.silu(gate) * upward).astype(jnp.bfloat16)
    flat_hidden = hidden.reshape(-1, hidden.shape[2])
    summed = lax.psum_scatter(
        jnp.einsum("fd,sf->ds", down_mat, flat_hidden, preferred_element_type=jnp.float32).astype(
            jnp.bfloat16
        ),
        "tp",
        scatter_dimension=0,
        tiled=True,
    )
    back = lax.all_to_all(summed, "ep", split_axis=1, concat_axis=1, tiled=True)
    picked = (
        jnp.take(back, slot_index, axis=1).astype(jnp.float32).reshape(-1, row_count, top_count)
    )
    combined = jnp.einsum("drk,rk->rd", picked, route_weights)
    return combined.astype(jnp.bfloat16)


def visit_order(n):
    def key(e):
        left = 2 * e < n
        if e in (0, n - 1):
            return lambda s: (False, abs(s - e))
        return lambda s: (s > e if left else s < e, -abs(s - e))

    return [sorted((s for s in range(n) if s != e), key=key(e)) for e in range(n)]


def fused_kernel(
    n,
    q_hbm,
    k_hbm,
    v_hbm,
    lam_hbm,
    hgain_hbm,
    tok_hbm,
    ids_hbm,
    rw_hbm,
    mgain_hbm,
    wg_hbm,
    wu_hbm,
    wd_hbm,
    heads_ref,
    out_ref,
    wg,
    wu,
    wd,
    q_ref,
    lam_ref,
    hgain_ref,
    tok_ref,
    ids_ref,
    rw_ref,
    mgain_ref,
    gathered,
    kv,
    hid,
    part,
    core_in,
    s_own,
    s_out,
    x_in,
    t_out,
    ret,
    z_out,
    z_in,
    join,
    lines,
    tables,
    own_weights,
    weights_at,
    wsem,
    tok_sem,
    in_sem,
    own_send,
    z_send,
    z_recv,
    x_send,
    x_recv,
    c_send,
    c_recv,
    kv_own_send,
    kv_send,
    kv_recv,
    r1_send,
    r1_recv,
    r2_send,
    r2_recv,
    r3_send,
    r3_recv,
    zo_send,
    zo_recv,
    join_send,
    join_recv,
    tab_send,
    tab_recv,
):
    e = lax.axis_index("ep")
    t = lax.axis_index("tp")
    xi = t // 2
    ci = lax.rem(t, 2)
    core_peer = {"tp": 2 * xi + 1 - ci}
    tx = 2 * (1 - xi) + ci
    x_peer = {"tp": tx}
    rows, width = tok_ref.shape
    cols = width // 4
    kv_rows = k_hbm.shape[0]
    has_left = e > 0
    has_right = e < n - 1
    inner = jnp.logical_and(has_left, has_right)
    outer = jnp.logical_not(inner)
    left_half = 2 * e < n
    inward = {"ep": jnp.clip(jnp.where(left_half, e + 1, e - 1), 0, n - 1)}
    outward = {"ep": jnp.clip(jnp.where(left_half, e - 1, e + 1), 0, n - 1)}

    def colblock(j):
        return pl.ds(pl.multiple_of(j * cols, 128), cols)

    def remote(src, dst, ss, rs, dev):
        return pltpu.make_async_remote_copy(
            src_ref=src, dst_ref=dst, send_sem=ss, recv_sem=rs, device_id=dev, device_id_type=MESH
        )

    barrier = pltpu.get_barrier_semaphore()
    pl.semaphore_signal(barrier, inc=1, device_id=inward, device_id_type=MESH)

    @pl.when(inner)
    def _():
        pl.semaphore_signal(barrier, inc=1, device_id=outward, device_id_type=MESH)

    pl.semaphore_signal(barrier, inc=1, device_id=core_peer, device_id_type=MESH)
    pl.semaphore_signal(barrier, inc=1, device_id=x_peer, device_id_type=MESH)
    greeted = 3 + inner.astype(jnp.int32)

    halves = range(PIECES)
    early, late = halves[: PIECES // 2], halves[PIECES // 2 :]
    hr = rows // PIECES

    def half(h):
        return pl.ds(h * hr, hr)

    own_kv = pl.ds(pl.multiple_of(e * kv_rows, kv_rows), kv_rows)
    k_width = k_hbm.shape[1]
    v_width = v_hbm.shape[1]
    gain_in = pltpu.make_async_copy(mgain_hbm, mgain_ref, in_sem.at[0])
    gain_in.start()
    tokens_in = [
        pltpu.make_async_copy(tok_hbm.at[half(h)], tok_ref.at[half(h)], tok_sem.at[h])
        for h in halves
    ]
    for c in tokens_in:
        c.start()
    weights = [
        pltpu.make_async_copy(a, b, wsem.at[i])
        for i, (a, b) in enumerate(((wg_hbm.at[0], wg), (wu_hbm.at[0], wu), (wd_hbm.at[0], wd)))
    ]
    kv_in = [
        pltpu.make_async_copy(k_hbm, kv.at[own_kv, pl.ds(0, k_width)], in_sem.at[1]),
        pltpu.make_async_copy(v_hbm, kv.at[own_kv, pl.ds(k_width, v_width)], in_sem.at[2]),
    ]
    others_in = [
        pltpu.make_async_copy(a, b, in_sem.at[i + 3])
        for i, (a, b) in enumerate(
            ((ids_hbm, ids_ref), (rw_hbm, rw_ref), (q_hbm, q_ref), (lam_hbm, lam_ref), (hgain_hbm, hgain_ref))
        )
    ]

    def normalize(h):
        step = 32

        @pl.loop(0, hr // step)
        def _(i):
            sl = pl.ds(pl.multiple_of(h * hr + i * step, step), step)
            v = tok_ref[sl, :].astype(F32)
            scale = lax.rsqrt(jnp.mean(v * v, axis=1, keepdims=True) + 1e-06)
            gathered[e, sl, :] = (v * scale * mgain_ref[...]).astype(BF16)

    def own_tok(side, h):
        blk = gathered.at[e, half(h), colblock(t)]
        return remote(blk, blk, own_send.at[0], z_recv.at[e, h], (inward, outward)[side])

    def own_tok2(h):
        blk = gathered.at[e, half(h), colblock(tx)]
        return remote(blk, blk, own_send.at[0], x_recv.at[e, h], inward)

    def own_kv_copy(side):
        blk = kv.at[own_kv]
        return remote(blk, blk, kv_own_send.at[0], kv_recv.at[e], (inward, outward)[side])

    orders = visit_order(n)

    def nth(k):
        s = jnp.int32(orders[0][k])
        for i in range(1, n):
            s = jnp.where(e == i, jnp.int32(orders[i][k]), s)
        return s

    visits = [nth(k) for k in range(n - 1)]

    def onward(k):
        return inward if k == OUTER_VISIT else outward

    def z_copy(k, h):
        blk = gathered.at[visits[k], half(h), colblock(t)]
        return remote(blk, blk, z_send.at[0], z_recv.at[visits[k], h], onward(k))

    def kv_copy(k):
        s = visits[k]
        blk = kv.at[pl.ds(pl.multiple_of(s * kv_rows, kv_rows), kv_rows)]
        return remote(blk, blk, kv_send.at[0], kv_recv.at[s], onward(k))

    def x_copy(s, h):
        blk = gathered.at[s, half(h), colblock(t)]
        return remote(blk, blk, x_send.at[0], x_recv.at[s, h], x_peer)

    def c_copy(s, h, which):
        blk = gathered.at[s, half(h), colblock((t, tx)[which])]
        return remote(blk, blk, c_send.at[0], c_recv.at[s], core_peer)

    def r1_copy(s, xx):
        return remote(
            part.at[s, :, colblock(2 * xx + 1 - ci)],
            core_in.at[s, xx],
            r1_send.at[0],
            r1_recv.at[xx, s],
            core_peer,
        )

    def r2_copy(s, h):
        return remote(
            s_out.at[s, half(h)], x_in.at[s, half(h)], r2_send.at[s], r2_recv.at[s, h], x_peer
        )

    def ret_copy(s, h):
        return remote(
            t_out.at[s, half(h)], ret.at[e, half(h)], r3_send.at[0], r3_recv.at[e], {"ep": s}
        )

    def join_copy(s, h):
        return remote(
            t_out.at[s, half(h)], join.at[half(h)], join_send.at[0], join_recv.at[h], inward
        )

    def tab_copy(s):
        return remote(lines, tables.at[e], tab_send.at[0], tab_recv.at[e], {"ep": s})

    def tab_back(s):
        return remote(lines, tables.at[s], tab_send.at[0], tab_recv.at[s], {"ep": s})

    def zo_copy(i, h):
        return remote(
            z_out.at[i, half(h)], z_in.at[i, half(h)], zo_send.at[0], zo_recv.at[0], inward
        )

    ff = wg.shape[1]
    nb = ff // 3

    def up_step(s, b):
        sl = pl.ds(b * nb, nb)
        g = jnp.dot(gathered[s], wg[:, sl], preferred_element_type=F32)
        u = jnp.dot(gathered[s], wu[:, sl], preferred_element_type=F32)
        hid[:, sl] = (g / (1.0 + jnp.exp(-g)) * u).astype(BF16)

    def down_step(s, j):
        sl = colblock(j)
        part[s, :, sl] = jnp.dot(hid[...], wd[:, sl], preferred_element_type=F32).astype(BF16)

    def down_far(s):
        down_step(s, 2 * (1 - xi) + 1 - ci)
        r1_copy(s, 1 - xi).start()
        down_step(s, tx)

    def down_near(s):
        down_step(s, 2 * xi + 1 - ci)
        r1_copy(s, xi).start()
        down_step(s, t)

    def across(s, h):
        return part[s, half(h), colblock(tx)].astype(F32) + core_in[s, 1 - xi, half(h)].astype(F32)

    def along(s, h):
        return part[s, half(h), colblock(t)].astype(F32) + core_in[s, xi, half(h)].astype(F32)

    def reduce_core(s):
        r1_copy(s, 1 - xi).wait_recv()
        for h in halves:
            s_out[s, half(h)] = across(s, h).astype(BF16)
            r2_copy(s, h).start()

    def reduce_z_far(s):
        r1_copy(s, 1 - xi).wait_recv()
        for h in halves:
            z_out[0, half(h)] = across(s, h).astype(BF16)
            zo_copy(0, h).start()

    def reduce_z_near(s):
        r1_copy(s, xi).wait_recv()
        for h in halves:
            z_out[1, half(h)] = along(s, h).astype(BF16)
            zo_copy(1, h).start()

    def take_zo():
        waiter(z_in, zo_send.at[0], zo_recv.at[0]).wait_recv()

    def own_sums():
        r1_copy(e, 1 - xi).wait_recv()
        r1_copy(e, xi).wait_recv()

    def reduce_own(h, joined):
        w = own_weights[half(h), 0:1]
        there = across(e, h) * w
        here = along(e, h) * w
        if joined:
            v = own_weights[half(h), 1:2]
            there = there + z_in[0, half(h)].astype(F32) * v
            here = here + z_in[1, half(h)].astype(F32) * v
        s_out[e, half(h)] = there.astype(BF16)
        r2_copy(e, h).start()
        s_own[half(h)] = here

    def finish(k, h, hand, joined=False):
        s = visits[k]
        if h == 0:
            r1_copy(s, xi).wait_recv()
        r2_copy(s, h).wait_recv()
        total = (along(s, h) + x_in[s, half(h)].astype(F32)) * weights_at[half(h), k : k + 1]
        if joined:
            join_copy(s, h).wait_recv()
            total = total + join[half(h)].astype(F32)
        t_out[s, half(h)] = total.astype(BF16)
        hand(s, h).start()

    def columns(picked):
        pad = jnp.zeros(((-len(picked)) % 8, rows), F32)
        return jnp.concatenate(picked + [pad], axis=0).T

    def line_of(table, x):
        is_x = lax.broadcasted_iota(jnp.int32, table.shape, 0) == x
        return jnp.sum(jnp.where(is_x, table, 0.0), axis=0, keepdims=True)

    def weigh():
        for s in visits:
            tab_back(s).wait_recv()
        weights_at[...] = columns([line_of(tables[s], e) for s in visits])

    def start_tables():
        for s in visits:
            tab_copy(s).start()

    def arrive(k, h, x=True):
        z_copy(k, h).wait_recv()
        if x:
            x_copy(visits[k], h).start()
        c_copy(visits[k], h, 0).start()

    def relay(k, h, x=True):
        z_copy(k, h).wait_recv()
        z_copy(k, h).start()
        if x:
            x_copy(visits[k], h).start()
        c_copy(visits[k], h, 0).start()

    def cross(k, h):
        x_copy(visits[k], h).wait_recv()
        c_copy(visits[k], h, 1).start()

    def waiter(ref, ss, rs):
        return remote(ref, ref, ss, rs, core_peer)

    def ready(s):
        waiter(gathered.at[s, :, pl.ds(0, 2 * cols)], c_send.at[0], c_recv.at[s]).wait_recv()

    def attend(h):
        heads = lam_ref.shape[0]
        vd = v_width // heads
        hd = q_ref.shape[1] // (2 * heads)
        qr = q_ref.shape[0]
        first = lax.broadcasted_iota(jnp.int32, (qr, 2 * hd), 1) < hd
        q = q_ref[:, h * 2 * hd : (h + 1) * 2 * hd].astype(F32)
        both = jnp.concatenate(
            [jnp.where(first, q, 0.0).astype(BF16), jnp.where(first, 0.0, q).astype(BF16)], axis=0
        )
        kh = kv[:, h * 2 * hd : (h + 1) * 2 * hd]
        vh = kv[:, k_width + h * vd : k_width + (h + 1) * vd]
        scores = lax.dot_general(
            both, kh, (((1,), (1,)), ((), ())), preferred_element_type=F32
        ) * (hd ** (-0.5))
        ex = jnp.exp(scores - jnp.max(scores, axis=1, keepdims=True))
        tot = jnp.sum(ex, axis=1, keepdims=True)
        sums = jnp.dot(ex.astype(BF16), vh, preferred_element_type=F32) / tot
        mixed = sums[:qr] - lam_ref[h] * sums[qr:]
        norm = lax.rsqrt(jnp.mean(mixed * mixed, axis=1, keepdims=True) + 1e-06)
        heads_ref[:, h * vd : (h + 1) * vd] = (mixed * norm * hgain_ref[...]).astype(BF16)

    def add_back(k, h, end):
        total = s_own[half(h)] + ret[visits[k], half(h)].astype(F32)
        if end:
            out_ref[half(h), :] = total.astype(BF16)
        else:
            s_own[half(h)] = total

    def drained(k):
        waiter(s_out.at[visits[k]], r2_send.at[visits[k]], r2_recv.at[visits[k], 0]).wait_send()

    def on_inner(fn):
        pl.when(inner)(fn)

    def on_outer(fn):
        pl.when(outer)(fn)

    def at(out, inn):
        if out:

            @on_outer
            def _():
                for f, *args in out:
                    f(*args)

        if inn:

            @on_inner
            def _():
                for f, *args in inn:
                    f(*args)

    def start_kv(side):
        own_kv_copy(side).start()

    def take_kv(k):
        kv_copy(k).wait_recv()

    def pass_kv(k):
        kv_copy(k).wait_recv()
        kv_copy(k).start()

    def start_tok2(h):
        own_tok2(h).start()

    def relays(h):
        relay(OUTER_VISIT, h, False)
        relay(2, h)

    gain_in.wait()
    for c in kv_in + others_in:
        c.start()
    for h in halves:
        if h == 0:
            tokens_in[h].wait()
        normalize(h)
        if h == 0:
            for c in tokens_in[1:]:
                c.wait()
            for c in weights:
                c.start()
            pl.semaphore_wait(barrier, greeted)
        own_tok(0, h).start()

        @on_inner
        def _():
            own_tok(1, h).start()

    for c in kv_in + others_in:
        c.wait()
    ids = ids_ref[...]
    rw = rw_ref[...]
    each = [jnp.sum(jnp.where(ids == x, rw, 0.0), axis=0, keepdims=True) for x in range(n)]
    lines[...] = jnp.concatenate(each + [jnp.zeros((lines.shape[0] - n, rows), F32)], axis=0)
    own_weights[...] = columns([line_of(lines[...], e), line_of(lines[...], visits[OUTER_VISIT])])

    for c in weights:
        c.wait()
    v0, v1, v2 = visits
    up_step(e, 0)
    at([(arrive, 0, 0), (start_tok2, 0)], [(relays, 0)])
    up_step(e, 1)
    at([(arrive, 0, 1), (start_tok2, 1)], [(relays, 1)])
    up_step(e, 2)
    at([(arrive, 0, 2), (start_tok2, 2)], [(relays, 2)])
    down_far(e)
    at(
        [(start_tok2, 3), (arrive, 0, 3), (start_kv, 0), (cross, 0, 0)],
        [(relays, 3), (cross, 0, 0)],
    )
    down_near(e)
    at(
        [
            (arrive, 1, 0), (cross, 0, 1), (arrive, 1, 1), (cross, 0, 2), (arrive, 1, 2),
            (cross, 0, 3),
        ],
        [
            (relay, 1, 0), (start_tables,), (cross, 0, 1), (cross, 2, 0), (relay, 1, 1),
            (cross, 0, 2), (cross, 2, 1), (relay, 1, 2), (cross, 0, 3), (cross, 2, 2), (start_kv, 0),
        ],
    )
    ready(v0)
    up_step(v0, 0)
    at([(arrive, 1, 3), (cross, 1, 0)], [(relay, 1, 3), (cross, 2, 3), (start_kv, 1), (cross, 1, 0)])
    up_step(v0, 1)
    at([(arrive, 2, 0), (start_tables,), (cross, 1, 1)], [(cross, 1, 1)])
    up_step(v0, 2)
    at([(arrive, 2, 1), (cross, 1, 2)], [(cross, 1, 2), (pass_kv, 0)])
    down_far(v0)
    at([(arrive, 2, 2), (cross, 1, 3)], [(cross, 1, 3)])
    down_near(v0)
    own_sums()
    at([(arrive, 2, 3), (reduce_z_far, v0)], [(reduce_core, v0)])
    ready(v1)
    up_step(v1, 0)
    at([(reduce_z_near, v0), (cross, 2, 0), (cross, 2, 1)], [(pass_kv, 2)])
    up_step(v1, 1)
    at([(cross, 2, 2)], [])
    up_step(v1, 2)
    at([], [(weigh,)])
    down_far(v1)
    at([(cross, 2, 3)], [(finish, 0, 0, ret_copy)])
    down_near(v1)
    reduce_core(v1)
    at([(weigh,)], [(finish, 0, 1, ret_copy), (pass_kv, 1)])
    ready(v2)
    up_step(v2, 0)
    at([], [(finish, 0, 2, ret_copy)])
    up_step(v2, 1)
    at([], [(finish, 0, 3, ret_copy)])
    up_step(v2, 2)
    down_far(v2)
    down_near(v2)
    reduce_core(v2)
    at([(finish, 1, h, join_copy) for h in halves], [(finish, 1, h, ret_copy) for h in halves])

    def attention():
        for k in range(n - 1):
            take_kv(k)
        for h in range(lam_ref.shape[0]):
            attend(h)

    def attention_here():
        for h in range(lam_ref.shape[0]):
            attend(h)

    at(
        [(finish, 2, h, ret_copy) for h in early] + [(drained, 2)]
        + [(reduce_own, h, False) for h in halves] + [(finish, 2, h, ret_copy) for h in late]
        + [(attention,)],
        [(finish, 2, h, ret_copy, True) for h in early] + [(drained, 2), (take_zo,)]
        + [(reduce_own, h, True) for h in halves]
        + [(finish, 2, h, ret_copy, True) for h in late] + [(attention_here,)],
    )

    for h in halves:
        r2_copy(e, h).wait_recv()
        s_own[half(h)] = s_own[half(h)] + x_in[e, half(h)].astype(F32)

    def gather_back(ks):
        for k in ks:
            waiter(ret.at[visits[k]], r3_send.at[0], r3_recv.at[visits[k]]).wait_recv()
            for h in halves:
                add_back(k, h, k == ks[-1])

    @on_outer
    def _():
        gather_back((0, 1, 2))

    @on_inner
    def _():
        gather_back((2,))

    def sent(ref, sem):
        waiter(ref, sem, c_recv.at[e]).wait_send()

    quarter, double = pl.ds(0, cols), pl.ds(0, 2 * cols)
    sent(part.at[:, :, double], r1_send.at[0])
    sent(gathered.at[pl.ds(0, 3), :, double], c_send.at[0])
    sent(gathered.at[pl.ds(0, 2), :, quarter], own_send.at[0])
    sent(s_out.at[e], r2_send.at[e])
    sent(tables.at[pl.ds(0, 3)], tab_send.at[0])
    sent(s_out.at[v1], r2_send.at[v1])

    @on_outer
    def _():
        sent(gathered.at[pl.ds(0, 3), :, quarter], x_send.at[0])
        sent(z_out, zo_send.at[0])
        sent(kv.at[pl.ds(0, kv_rows)], kv_own_send.at[0])
        sent(t_out.at[0], r3_send.at[0])
        sent(t_out.at[0], join_send.at[0])

    @on_inner
    def _():
        sent(kv.at[pl.ds(0, 2 * kv_rows)], kv_own_send.at[0])
        sent(kv.at[pl.ds(0, 3 * kv_rows)], kv_send.at[0])
        sent(gathered.at[pl.ds(0, 3), :, quarter], z_send.at[0])
        sent(gathered.at[pl.ds(0, 2), :, quarter], x_send.at[0])
        sent(s_out.at[v0], r2_send.at[v0])
        sent(t_out.at[pl.ds(0, 3)], r3_send.at[0])


def hand_on_kernel(a_ref, b_ref, c_ref, d_ref):
    c_ref[...] = a_ref[...]
    d_ref[...] = b_ref[...]


def fused(queries, keys, values, lambdas, head_gain, tokens, route_ids, route_weights, moe_gain, w_gate, w_up, w_down):
    n = lax.axis_size("ep")
    rows, width = tokens.shape
    cols = width // 4
    ff = w_gate.shape[2]
    vmem = pl.BlockSpec(memory_space=pltpu.VMEM)
    hbm = pl.BlockSpec(memory_space=pltpu.HBM)
    dma = pltpu.SemaphoreType.DMA
    results = pl.pallas_call(
        functools.partial(fused_kernel, n),
        out_shape=(
            pltpu.VMEM((queries.shape[0], values.shape[1]), BF16),
            pltpu.VMEM((rows, cols), BF16),
        ),
        in_specs=[hbm] * 12,
        out_specs=(vmem, vmem),
        scratch_shapes=[
            pltpu.VMEM((width, ff), BF16),
            pltpu.VMEM((width, ff), BF16),
            pltpu.VMEM((ff, width), BF16),
            pltpu.VMEM(queries.shape, BF16),
            pltpu.SMEM(lambdas.shape, F32),
            pltpu.VMEM(head_gain.shape, F32),
            pltpu.VMEM((rows, width), BF16),
            pltpu.VMEM(route_ids.shape[::-1], jnp.int32),
            pltpu.VMEM(route_weights.shape[::-1], F32),
            pltpu.VMEM(moe_gain.shape, F32),
            pltpu.VMEM((n, rows, width), BF16),
            pltpu.VMEM((n * keys.shape[0], keys.shape[1] + values.shape[1]), BF16),
            pltpu.VMEM((rows, ff), BF16),
            pltpu.VMEM((n, rows, width), BF16),
            pltpu.VMEM((n, 2, rows, cols), BF16),
            pltpu.VMEM((rows, cols), F32),
            pltpu.VMEM((n, rows, cols), BF16),
            pltpu.VMEM((n, rows, cols), BF16),
            pltpu.VMEM((n, rows, cols), BF16),
            pltpu.VMEM((n, rows, cols), BF16),
            pltpu.VMEM((2, rows, cols), BF16),
            pltpu.VMEM((2, rows, cols), BF16),
            pltpu.VMEM((rows, cols), BF16),
            pltpu.VMEM((-(-n // 8) * 8, rows), F32),
            pltpu.VMEM((n, -(-n // 8) * 8, rows), F32),
            pltpu.VMEM((rows, 8), F32),
            pltpu.VMEM((rows, 8), F32),
            dma((3,)),
            dma((PIECES,)),
            dma((8,)),
            dma((1,)),
            dma((1,)),
            dma((n, PIECES)),
            dma((1,)),
            dma((n, PIECES)),
            dma((1,)),
            dma((n,)),
            dma((1,)),
            dma((1,)),
            dma((n,)),
            dma((1,)),
            dma((2, n)),
            dma((n,)),
            dma((n, PIECES)),
            dma((1,)),
            dma((n,)),
            dma((1,)),
            dma((1,)),
            dma((1,)),
            dma((PIECES,)),
            dma((1,)),
            dma((n,)),
        ],
        compiler_params=pltpu.CompilerParams(
            collective_id=0, has_side_effects=True, vmem_limit_bytes=60 * 1024 * 1024
        ),
        name="fused_layer",
    )(
        queries,
        keys,
        values,
        lambdas,
        head_gain,
        tokens,
        route_ids.T,
        route_weights.T,
        moe_gain,
        w_gate,
        w_up,
        w_down,
    )
    return pl.pallas_call(
        hand_on_kernel,
        out_shape=tuple(jax.ShapeDtypeStruct(r.shape, r.dtype) for r in results),
        in_specs=[vmem, vmem],
        out_specs=(vmem, vmem),
        compiler_params=pltpu.CompilerParams(vmem_limit_bytes=4 * 1024 * 1024),
        name="hand_on",
    )(*results)


def on_device(
    queries,
    keys,
    values,
    lambdas,
    head_gain,
    tokens,
    route_ids,
    route_weights,
    moe_gain,
    w_gate,
    w_up,
    w_down,
):
    rows = tokens.shape[0]
    expert_count = w_gate.shape[0] * lax.axis_size("ep")
    slots = 2 * rows * route_ids.shape[1] // expert_count
    if w_gate.shape[0] == 1 and lax.axis_size("tp") == lax.axis_size("ep") == 4 and slots >= rows:
        return fused(
            queries, keys, values, lambdas, head_gain, tokens,
            route_ids, route_weights, moe_gain, w_gate, w_up, w_down,
        )
    heads_out = attend(queries, keys, values, lambdas, head_gain)
    expert_out = experts(tokens, route_ids, route_weights, moe_gain, w_gate, w_up, w_down)
    return (heads_out, expert_out)


def solution(mesh):
    in_specs = (
        P(("grp", "ep"), "tp"),
        P(("grp", "ep"), "tp"),
        P(("grp", "ep"), "tp"),
        P("tp"),
        P(),
        P(("grp", "ep"), None),
        P(("grp", "ep"), None),
        P(("grp", "ep"), None),
        P(),
        P("ep", None, "tp"),
        P("ep", None, "tp"),
        P("ep", "tp", None),
    )
    out_specs = (P(("grp", "ep"), "tp"), P(("grp", "ep"), "tp"))
    return jax.shard_map(
        on_device, mesh=mesh, in_specs=in_specs, out_specs=out_specs, check_vma=False
    )
```

```python
import functools

import jax
import jax.numpy as jnp
from jax import lax
from jax.experimental import pallas as pl
from jax.experimental.pallas import tpu as pltpu
from jax.sharding import PartitionSpec as P

MESH = pl.DeviceIdType.MESH
F32 = jnp.float32
BF16 = jnp.bfloat16
PIECES = 4
OUTER_VISIT = 0

def attend(queries, keys, values, lambdas, head_gain):
    row_count = queries.shape[0]
    head_count = lambdas.shape[0]
    head_dim = queries.shape[1] // (2 * head_count)
    value_dim = values.shape[1] // head_count
    query_parts = queries.reshape(row_count, head_count, 2, head_dim)
    score_scale = head_dim ** (-0.5)
    running = jnp.full((head_count, 2, row_count), -1e30, jnp.float32)
    key_piece = lax.all_gather(keys, "ep", axis=0, tiled=True)
    value_piece = lax.all_gather(values, "ep", axis=0, tiled=True)
    count = key_piece.shape[0]
    key_parts = key_piece.reshape(count, head_count, 2, head_dim)
    value_parts = value_piece.reshape(count, head_count, value_dim)
    scores = (
        jnp.einsum("qhcd,khcd->hcqk", query_parts, key_parts, preferred_element_type=jnp.float32)
        * score_scale
    )
    newest = jnp.maximum(running, jnp.max(scores, axis=-1))
    weights_now = jnp.exp(scores - newest[..., None])
    totals = jnp.sum(weights_now, axis=-1)
    sums = jnp.einsum(
        "hcqk,khe->hcqe",
        weights_now.astype(jnp.bfloat16),
        value_parts,
        preferred_element_type=jnp.float32,
    )
    running, totals, sums = (newest, totals, sums)
    means = sums / totals[..., None]
    mixed = means[:, 0] - lambdas[:, None, None] * means[:, 1]
    scaled = mixed * lax.rsqrt(jnp.mean(mixed * mixed, axis=-1, keepdims=True) + 1e-06) * head_gain
    return (
        jnp.transpose(scaled, (1, 0, 2))
        .reshape(row_count, head_count * value_dim)
        .astype(jnp.bfloat16)
    )


def experts(tokens, route_ids, route_weights, moe_gain, w_gate, w_up, w_down):
    row_count, width = tokens.shape
    top_count = route_ids.shape[1]
    ep_size = lax.axis_size("ep")
    tp_size = lax.axis_size("tp")
    expert_count = w_gate.shape[0] * ep_size
    capacity = 2 * row_count * top_count // expert_count
    token_float = tokens.astype(jnp.float32)
    normed = (
        token_float
        * lax.rsqrt(jnp.mean(token_float * token_float, axis=1, keepdims=True) + 1e-06)
        * moe_gain
    ).astype(jnp.bfloat16)
    flat_ids = route_ids.reshape(-1)
    onehot = (flat_ids[:, None] == jnp.arange(expert_count, dtype=jnp.int32)[None, :]).astype(
        jnp.int32
    )
    earlier = jnp.cumsum(onehot, axis=0) - onehot
    position = jnp.sum(earlier * onehot, axis=1)
    slot_index = flat_ids * capacity + position
    owners = (
        jnp.full((expert_count * capacity,), row_count, jnp.int32)
        .at[slot_index]
        .set(jnp.arange(row_count * top_count, dtype=jnp.int32) // top_count)
    )
    padded = jnp.concatenate([normed, jnp.zeros((1, width), jnp.bfloat16)], axis=0)
    outgoing = padded[owners].reshape(expert_count, capacity, width)
    gate_mat = w_gate[0]
    up_mat = w_up[0]
    down_mat = w_down[0]
    slice_width = width // tp_size
    own_columns = lax.dynamic_slice_in_dim(
        outgoing, lax.axis_index("tp") * slice_width, slice_width, 2
    )
    arrived = lax.all_to_all(own_columns, "ep", split_axis=0, concat_axis=0, tiled=True)
    piece = lax.all_gather(arrived, "tp", axis=2, tiled=True)
    gate = jnp.einsum("scd,df->scf", piece, gate_mat, preferred_element_type=jnp.float32)
    upward = jnp.einsum("scd,df->scf", piece, up_mat, preferred_element_type=jnp.float32)
    hidden = (jax.nn.silu(gate) * upward).astype(jnp.bfloat16)
    flat_hidden = hidden.reshape(-1, hidden.shape[2])
    summed = lax.psum_scatter(
        jnp.einsum("fd,sf->ds", down_mat, flat_hidden, preferred_element_type=jnp.float32).astype(
            jnp.bfloat16
        ),
        "tp",
        scatter_dimension=0,
        tiled=True,
    )
    back = lax.all_to_all(summed, "ep", split_axis=1, concat_axis=1, tiled=True)
    picked = (
        jnp.take(back, slot_index, axis=1).astype(jnp.float32).reshape(-1, row_count, top_count)
    )
    combined = jnp.einsum("drk,rk->rd", picked, route_weights)
    return combined.astype(jnp.bfloat16)


def visit_order(n):
    def key(e):
        left = 2 * e < n
        if e in (0, n - 1):
            return lambda s: (False, abs(s - e))
        return lambda s: (s > e if left else s < e, -abs(s - e))

    return [sorted((s for s in range(n) if s != e), key=key(e)) for e in range(n)]


def fused_kernel(
    n,
    q_hbm,
    k_hbm,
    v_hbm,
    lam_hbm,
    hgain_hbm,
    tok_hbm,
    ids_hbm,
    rw_hbm,
    mgain_hbm,
    wg_hbm,
    wu_hbm,
    wd_hbm,
    heads_ref,
    out_ref,
    wg,
    wu,
    wd,
    q_ref,
    lam_ref,
    hgain_ref,
    tok_ref,
    ids_ref,
    rw_ref,
    mgain_ref,
    gathered,
    kv,
    hid,
    part,
    core_in,
    s_own,
    s_out,
    x_in,
    t_out,
    ret,
    z_out,
    z_in,
    join,
    lines,
    tables,
    own_weights,
    weights_at,
    wsem,
    tok_sem,
    in_sem,
    own_send,
    z_send,
    z_recv,
    x_send,
    x_recv,
    c_send,
    c_recv,
    kv_own_send,
    kv_send,
    kv_recv,
    r1_send,
    r1_recv,
    r2_send,
    r2_recv,
    r3_send,
    r3_recv,
    zo_send,
    zo_recv,
    join_send,
    join_recv,
    tab_send,
    tab_recv,
):
    e = lax.axis_index("ep")
    t = lax.axis_index("tp")
    xi = t // 2
    ci = lax.rem(t, 2)
    core_peer = {"tp": 2 * xi + 1 - ci}
    tx = 2 * (1 - xi) + ci
    x_peer = {"tp": tx}
    rows, width = tok_ref.shape
    cols = width // 4
    kv_rows = k_hbm.shape[0]
    has_left = e > 0
    has_right = e < n - 1
    inner = jnp.logical_and(has_left, has_right)
    outer = jnp.logical_not(inner)
    left_half = 2 * e < n
    inward = {"ep": jnp.clip(jnp.where(left_half, e + 1, e - 1), 0, n - 1)}
    outward = {"ep": jnp.clip(jnp.where(left_half, e - 1, e + 1), 0, n - 1)}

    def colblock(j):
        return pl.ds(pl.multiple_of(j * cols, 128), cols)

    def remote(src, dst, ss, rs, dev):
        return pltpu.make_async_remote_copy(
            src_ref=src, dst_ref=dst, send_sem=ss, recv_sem=rs, device_id=dev, device_id_type=MESH
        )

    barrier = pltpu.get_barrier_semaphore()
    pl.semaphore_signal(barrier, inc=1, device_id=inward, device_id_type=MESH)

    @pl.when(inner)
    def _():
        pl.semaphore_signal(barrier, inc=1, device_id=outward, device_id_type=MESH)

    pl.semaphore_signal(barrier, inc=1, device_id=core_peer, device_id_type=MESH)
    pl.semaphore_signal(barrier, inc=1, device_id=x_peer, device_id_type=MESH)
    greeted = 3 + inner.astype(jnp.int32)

    halves = range(PIECES)
    early, late = halves[: PIECES // 2], halves[PIECES // 2 :]
    hr = rows // PIECES

    def half(h):
        return pl.ds(h * hr, hr)

    own_kv = pl.ds(pl.multiple_of(e * kv_rows, kv_rows), kv_rows)
    k_width = k_hbm.shape[1]
    v_width = v_hbm.shape[1]
    gain_in = pltpu.make_async_copy(mgain_hbm, mgain_ref, in_sem.at[0])
    gain_in.start()
    tokens_in = [
        pltpu.make_async_copy(tok_hbm.at[half(h)], tok_ref.at[half(h)], tok_sem.at[h])
        for h in halves
    ]
    for c in tokens_in:
        c.start()
    weights = [
        pltpu.make_async_copy(a, b, wsem.at[i])
        for i, (a, b) in enumerate(((wg_hbm.at[0], wg), (wu_hbm.at[0], wu), (wd_hbm.at[0], wd)))
    ]
    kv_in = [
        pltpu.make_async_copy(k_hbm, kv.at[own_kv, pl.ds(0, k_width)], in_sem.at[1]),
        pltpu.make_async_copy(v_hbm, kv.at[own_kv, pl.ds(k_width, v_width)], in_sem.at[2]),
    ]
    others_in = [
        pltpu.make_async_copy(a, b, in_sem.at[i + 3])
        for i, (a, b) in enumerate(
            ((ids_hbm, ids_ref), (rw_hbm, rw_ref), (q_hbm, q_ref), (lam_hbm, lam_ref), (hgain_hbm, hgain_ref))
        )
    ]

    def normalize(h):
        step = 32

        @pl.loop(0, hr // step)
        def _(i):
            sl = pl.ds(pl.multiple_of(h * hr + i * step, step), step)
            v = tok_ref[sl, :].astype(F32)
            scale = lax.rsqrt(jnp.mean(v * v, axis=1, keepdims=True) + 1e-06)
            gathered[e, sl, :] = (v * scale * mgain_ref[...]).astype(BF16)

    def own_tok(side, h):
        blk = gathered.at[e, half(h), colblock(t)]
        return remote(blk, blk, own_send.at[0], z_recv.at[e, h], (inward, outward)[side])

    def own_tok2(h):
        blk = gathered.at[e, half(h), colblock(tx)]
        return remote(blk, blk, own_send.at[0], x_recv.at[e, h], inward)

    def own_kv_copy(side):
        blk = kv.at[own_kv]
        return remote(blk, blk, kv_own_send.at[0], kv_recv.at[e], (inward, outward)[side])

    orders = visit_order(n)

    def nth(k):
        s = jnp.int32(orders[0][k])
        for i in range(1, n):
            s = jnp.where(e == i, jnp.int32(orders[i][k]), s)
        return s

    visits = [nth(k) for k in range(n - 1)]

    def onward(k):
        return inward if k == OUTER_VISIT else outward

    def z_copy(k, h):
        blk = gathered.at[visits[k], half(h), colblock(t)]
        return remote(blk, blk, z_send.at[0], z_recv.at[visits[k], h], onward(k))

    def kv_copy(k):
        s = visits[k]
        blk = kv.at[pl.ds(pl.multiple_of(s * kv_rows, kv_rows), kv_rows)]
        return remote(blk, blk, kv_send.at[0], kv_recv.at[s], onward(k))

    def x_copy(s, h):
        blk = gathered.at[s, half(h), colblock(t)]
        return remote(blk, blk, x_send.at[0], x_recv.at[s, h], x_peer)

    def c_copy(s, h, which):
        blk = gathered.at[s, half(h), colblock((t, tx)[which])]
        return remote(blk, blk, c_send.at[0], c_recv.at[s], core_peer)

    def r1_copy(s, xx):
        return remote(
            part.at[s, :, colblock(2 * xx + 1 - ci)],
            core_in.at[s, xx],
            r1_send.at[0],
            r1_recv.at[xx, s],
            core_peer,
        )

    def r2_copy(s, h):
        return remote(
            s_out.at[s, half(h)], x_in.at[s, half(h)], r2_send.at[s], r2_recv.at[s, h], x_peer
        )

    def ret_copy(s, h):
        return remote(
            t_out.at[s, half(h)], ret.at[e, half(h)], r3_send.at[0], r3_recv.at[e], {"ep": s}
        )

    def join_copy(s, h):
        return remote(
            t_out.at[s, half(h)], join.at[half(h)], join_send.at[0], join_recv.at[h], inward
        )

    def tab_copy(s):
        return remote(lines, tables.at[e], tab_send.at[0], tab_recv.at[e], {"ep": s})

    def tab_back(s):
        return remote(lines, tables.at[s], tab_send.at[0], tab_recv.at[s], {"ep": s})

    def zo_copy(i, h):
        return remote(
            z_out.at[i, half(h)], z_in.at[i, half(h)], zo_send.at[0], zo_recv.at[0], inward
        )

    ff = wg.shape[1]
    nb = ff // 3

    def up_step(s, b):
        sl = pl.ds(b * nb, nb)
        g = jnp.dot(gathered[s], wg[:, sl], preferred_element_type=F32)
        u = jnp.dot(gathered[s], wu[:, sl], preferred_element_type=F32)
        hid[:, sl] = (g / (1.0 + jnp.exp(-g)) * u).astype(BF16)

    def down_step(s, j):
        sl = colblock(j)
        part[s, :, sl] = jnp.dot(hid[...], wd[:, sl], preferred_element_type=F32).astype(BF16)

    def down_far(s):
        down_step(s, 2 * (1 - xi) + 1 - ci)
        r1_copy(s, 1 - xi).start()
        down_step(s, tx)

    def down_near(s):
        down_step(s, 2 * xi + 1 - ci)
        r1_copy(s, xi).start()
        down_step(s, t)

    def across(s, h):
        return part[s, half(h), colblock(tx)].astype(F32) + core_in[s, 1 - xi, half(h)].astype(F32)

    def along(s, h):
        return part[s, half(h), colblock(t)].astype(F32) + core_in[s, xi, half(h)].astype(F32)

    def exchange(s, h):
        if h == 0:
            r1_copy(s, 1 - xi).wait_recv()
        s_out[s, half(h)] = across(s, h).astype(BF16)
        r2_copy(s, h).start()

    def reduce_z_far(s):
        r1_copy(s, 1 - xi).wait_recv()
        for h in halves:
            z_out[0, half(h)] = across(s, h).astype(BF16)
            zo_copy(0, h).start()

    def reduce_z_near(s):
        r1_copy(s, xi).wait_recv()
        for h in halves:
            z_out[1, half(h)] = along(s, h).astype(BF16)
            zo_copy(1, h).start()

    def take_zo():
        waiter(z_in, zo_send.at[0], zo_recv.at[0]).wait_recv()

    def own_sums():
        r1_copy(e, 1 - xi).wait_recv()
        r1_copy(e, xi).wait_recv()

    def reduce_own(h, joined):
        w = own_weights[half(h), 0:1]
        there = across(e, h) * w
        here = along(e, h) * w
        if joined:
            v = own_weights[half(h), 1:2]
            there = there + z_in[0, half(h)].astype(F32) * v
            here = here + z_in[1, half(h)].astype(F32) * v
        s_out[e, half(h)] = there.astype(BF16)
        r2_copy(e, h).start()
        s_own[half(h)] = here

    def finish(k, h, hand, joined=False):
        s = visits[k]
        if h == 0:
            r1_copy(s, xi).wait_recv()
        r2_copy(s, h).wait_recv()
        total = (along(s, h) + x_in[s, half(h)].astype(F32)) * weights_at[half(h), k : k + 1]
        if joined:
            join_copy(s, h).wait_recv()
            total = total + join[half(h)].astype(F32)
        t_out[s, half(h)] = total.astype(BF16)
        hand(s, h).start()

    def columns(picked):
        pad = jnp.zeros(((-len(picked)) % 8, rows), F32)
        return jnp.concatenate(picked + [pad], axis=0).T

    def line_of(table, x):
        is_x = lax.broadcasted_iota(jnp.int32, table.shape, 0) == x
        return jnp.sum(jnp.where(is_x, table, 0.0), axis=0, keepdims=True)

    def weigh():
        for s in visits:
            tab_back(s).wait_recv()
        weights_at[...] = columns([line_of(tables[s], e) for s in visits])

    def start_tables():
        for s in visits:
            tab_copy(s).start()

    def arrive(k, h, x=True):
        z_copy(k, h).wait_recv()
        if x:
            x_copy(visits[k], h).start()
        c_copy(visits[k], h, 0).start()

    def relay(k, h, x=True):
        z_copy(k, h).wait_recv()
        z_copy(k, h).start()
        if x:
            x_copy(visits[k], h).start()
        c_copy(visits[k], h, 0).start()

    def cross(k, h):
        x_copy(visits[k], h).wait_recv()
        c_copy(visits[k], h, 1).start()

    def waiter(ref, ss, rs):
        return remote(ref, ref, ss, rs, core_peer)

    def ready(s):
        waiter(gathered.at[s, :, pl.ds(0, 2 * cols)], c_send.at[0], c_recv.at[s]).wait_recv()

    def attend(h):
        heads = lam_ref.shape[0]
        vd = v_width // heads
        hd = q_ref.shape[1] // (2 * heads)
        qr = q_ref.shape[0]
        first = lax.broadcasted_iota(jnp.int32, (qr, 2 * hd), 1) < hd
        q = q_ref[:, h * 2 * hd : (h + 1) * 2 * hd].astype(F32)
        both = jnp.concatenate(
            [jnp.where(first, q, 0.0).astype(BF16), jnp.where(first, 0.0, q).astype(BF16)], axis=0
        )
        kh = kv[:, h * 2 * hd : (h + 1) * 2 * hd]
        vh = kv[:, k_width + h * vd : k_width + (h + 1) * vd]
        scores = lax.dot_general(
            both, kh, (((1,), (1,)), ((), ())), preferred_element_type=F32
        ) * (hd ** (-0.5))
        ex = jnp.exp(scores - jnp.max(scores, axis=1, keepdims=True))
        tot = jnp.sum(ex, axis=1, keepdims=True)
        sums = jnp.dot(ex.astype(BF16), vh, preferred_element_type=F32) / tot
        mixed = sums[:qr] - lam_ref[h] * sums[qr:]
        norm = lax.rsqrt(jnp.mean(mixed * mixed, axis=1, keepdims=True) + 1e-06)
        heads_ref[:, h * vd : (h + 1) * vd] = (mixed * norm * hgain_ref[...]).astype(BF16)

    def add_back(k, h, end):
        total = s_own[half(h)] + ret[visits[k], half(h)].astype(F32)
        if end:
            out_ref[half(h), :] = total.astype(BF16)
        else:
            s_own[half(h)] = total

    def drained(k):
        waiter(s_out.at[visits[k]], r2_send.at[visits[k]], r2_recv.at[visits[k], 0]).wait_send()

    def on_inner(fn):
        pl.when(inner)(fn)

    def on_outer(fn):
        pl.when(outer)(fn)

    def at(out, inn):
        if out:

            @on_outer
            def _():
                for f, *args in out:
                    f(*args)

        if inn:

            @on_inner
            def _():
                for f, *args in inn:
                    f(*args)

    def start_kv(side):
        own_kv_copy(side).start()

    def take_kv(k):
        kv_copy(k).wait_recv()

    def pass_kv(k):
        kv_copy(k).wait_recv()
        kv_copy(k).start()

    def start_tok2(h):
        own_tok2(h).start()

    def relays(h):
        relay(OUTER_VISIT, h, False)
        relay(2, h)

    gain_in.wait()
    for c in kv_in + others_in:
        c.start()
    for h in halves:
        if h == 0:
            tokens_in[h].wait()
        normalize(h)
        if h == 0:
            for c in tokens_in[1:]:
                c.wait()
            for c in weights:
                c.start()
            pl.semaphore_wait(barrier, greeted)
        own_tok(0, h).start()

        @on_inner
        def _():
            own_tok(1, h).start()

    for c in kv_in + others_in:
        c.wait()
    ids = ids_ref[...]
    rw = rw_ref[...]
    each = [jnp.sum(jnp.where(ids == x, rw, 0.0), axis=0, keepdims=True) for x in range(n)]
    lines[...] = jnp.concatenate(each + [jnp.zeros((lines.shape[0] - n, rows), F32)], axis=0)
    own_weights[...] = columns([line_of(lines[...], e), line_of(lines[...], visits[OUTER_VISIT])])

    for c in weights:
        c.wait()
    v0, v1, v2 = visits
    up_step(e, 0)
    at([(arrive, 0, 0), (start_tok2, 0)], [(relays, 0)])
    up_step(e, 1)
    at([(arrive, 0, 1), (start_tok2, 1)], [(relays, 1)])
    up_step(e, 2)
    at([(arrive, 0, 2), (start_tok2, 2)], [(relays, 2)])
    down_far(e)
    at(
        [(start_tok2, 3), (arrive, 0, 3), (start_kv, 0), (cross, 0, 0)],
        [(relays, 3), (cross, 0, 0)],
    )
    down_near(e)
    at(
        [
            (arrive, 1, 0), (cross, 0, 1), (arrive, 1, 1), (cross, 0, 2), (arrive, 1, 2),
            (cross, 0, 3),
        ],
        [
            (relay, 1, 0), (start_tables,), (cross, 0, 1), (cross, 2, 0), (relay, 1, 1),
            (cross, 0, 2), (cross, 2, 1), (relay, 1, 2), (cross, 0, 3), (cross, 2, 2), (start_kv, 0),
        ],
    )
    ready(v0)
    up_step(v0, 0)
    at([(arrive, 1, 3), (cross, 1, 0)], [(relay, 1, 3), (cross, 2, 3), (start_kv, 1), (cross, 1, 0)])
    up_step(v0, 1)
    at([(arrive, 2, 0), (start_tables,), (cross, 1, 1)], [(cross, 1, 1)])
    up_step(v0, 2)
    at([(arrive, 2, 1), (cross, 1, 2)], [(cross, 1, 2), (pass_kv, 0)])
    down_far(v0)
    at([(arrive, 2, 2), (cross, 1, 3)], [(cross, 1, 3)])
    down_near(v0)
    own_sums()
    at([(arrive, 2, 3), (reduce_z_far, v0)], [(exchange, v0, 0)])
    ready(v1)
    up_step(v1, 0)
    at(
        [(reduce_z_near, v0), (cross, 2, 0), (cross, 2, 1)],
        [(exchange, v0, 1), (pass_kv, 2)],
    )
    up_step(v1, 1)
    at([(cross, 2, 2)], [(exchange, v0, 2)])
    up_step(v1, 2)
    at([], [(exchange, v0, 3), (weigh,)])
    down_far(v1)
    at([(cross, 2, 3)], [(finish, 0, 0, ret_copy)])
    down_near(v1)
    exchange(v1, 0)
    at([(weigh,)], [(finish, 0, 1, ret_copy), (pass_kv, 1)])
    ready(v2)
    up_step(v2, 0)
    exchange(v1, 1)
    at([], [(finish, 0, 2, ret_copy)])
    up_step(v2, 1)
    exchange(v1, 2)
    up_step(v2, 2)
    exchange(v1, 3)
    at([], [(finish, 0, 3, ret_copy)])
    down_far(v2)
    at([], [(finish, 1, 0, ret_copy)])
    down_near(v2)
    exchange(v2, 0)
    for h in halves:
        at(
            [(finish, 1, h, join_copy)],
            [(finish, 1, h, ret_copy)] if h else [],
        )
        if h + 1 < PIECES:
            exchange(v2, h + 1)

    def attention():
        for k in range(n - 1):
            take_kv(k)
        for h in range(lam_ref.shape[0]):
            attend(h)

    def attention_here():
        for h in range(lam_ref.shape[0]):
            attend(h)

    at(
        [(finish, 2, h, ret_copy) for h in early] + [(drained, 2)]
        + [(reduce_own, h, False) for h in halves] + [(finish, 2, h, ret_copy) for h in late]
        + [(attention,)],
        [(finish, 2, h, ret_copy, True) for h in early] + [(drained, 2), (take_zo,)]
        + [(reduce_own, h, True) for h in halves]
        + [(finish, 2, h, ret_copy, True) for h in late] + [(attention_here,)],
    )

    for h in halves:
        r2_copy(e, h).wait_recv()
        s_own[half(h)] = s_own[half(h)] + x_in[e, half(h)].astype(F32)

    def gather_back(ks):
        for k in ks:
            waiter(ret.at[visits[k]], r3_send.at[0], r3_recv.at[visits[k]]).wait_recv()
            for h in halves:
                add_back(k, h, k == ks[-1])

    @on_outer
    def _():
        gather_back((0, 1, 2))

    @on_inner
    def _():
        gather_back((2,))

    def sent(ref, sem):
        waiter(ref, sem, c_recv.at[e]).wait_send()

    quarter, double = pl.ds(0, cols), pl.ds(0, 2 * cols)
    sent(part.at[:, :, double], r1_send.at[0])
    sent(gathered.at[pl.ds(0, 3), :, double], c_send.at[0])
    sent(gathered.at[pl.ds(0, 2), :, quarter], own_send.at[0])
    sent(s_out.at[e], r2_send.at[e])
    sent(tables.at[pl.ds(0, 3)], tab_send.at[0])
    sent(s_out.at[v1], r2_send.at[v1])

    @on_outer
    def _():
        sent(gathered.at[pl.ds(0, 3), :, quarter], x_send.at[0])
        sent(z_out, zo_send.at[0])
        sent(kv.at[pl.ds(0, kv_rows)], kv_own_send.at[0])
        sent(t_out.at[0], r3_send.at[0])
        sent(t_out.at[0], join_send.at[0])

    @on_inner
    def _():
        sent(kv.at[pl.ds(0, 2 * kv_rows)], kv_own_send.at[0])
        sent(kv.at[pl.ds(0, 3 * kv_rows)], kv_send.at[0])
        sent(gathered.at[pl.ds(0, 3), :, quarter], z_send.at[0])
        sent(gathered.at[pl.ds(0, 2), :, quarter], x_send.at[0])
        sent(s_out.at[v0], r2_send.at[v0])
        sent(t_out.at[pl.ds(0, 3)], r3_send.at[0])


def hand_on_kernel(a_ref, b_ref, c_ref, d_ref):
    c_ref[...] = a_ref[...]
    d_ref[...] = b_ref[...]


def fused(queries, keys, values, lambdas, head_gain, tokens, route_ids, route_weights, moe_gain, w_gate, w_up, w_down):
    n = lax.axis_size("ep")
    rows, width = tokens.shape
    cols = width // 4
    ff = w_gate.shape[2]
    vmem = pl.BlockSpec(memory_space=pltpu.VMEM)
    hbm = pl.BlockSpec(memory_space=pltpu.HBM)
    dma = pltpu.SemaphoreType.DMA
    results = pl.pallas_call(
        functools.partial(fused_kernel, n),
        out_shape=(
            pltpu.VMEM((queries.shape[0], values.shape[1]), BF16),
            pltpu.VMEM((rows, cols), BF16),
        ),
        in_specs=[hbm] * 12,
        out_specs=(vmem, vmem),
        scratch_shapes=[
            pltpu.VMEM((width, ff), BF16),
            pltpu.VMEM((width, ff), BF16),
            pltpu.VMEM((ff, width), BF16),
            pltpu.VMEM(queries.shape, BF16),
            pltpu.SMEM(lambdas.shape, F32),
            pltpu.VMEM(head_gain.shape, F32),
            pltpu.VMEM((rows, width), BF16),
            pltpu.VMEM(route_ids.shape[::-1], jnp.int32),
            pltpu.VMEM(route_weights.shape[::-1], F32),
            pltpu.VMEM(moe_gain.shape, F32),
            pltpu.VMEM((n, rows, width), BF16),
            pltpu.VMEM((n * keys.shape[0], keys.shape[1] + values.shape[1]), BF16),
            pltpu.VMEM((rows, ff), BF16),
            pltpu.VMEM((n, rows, width), BF16),
            pltpu.VMEM((n, 2, rows, cols), BF16),
            pltpu.VMEM((rows, cols), F32),
            pltpu.VMEM((n, rows, cols), BF16),
            pltpu.VMEM((n, rows, cols), BF16),
            pltpu.VMEM((n, rows, cols), BF16),
            pltpu.VMEM((n, rows, cols), BF16),
            pltpu.VMEM((2, rows, cols), BF16),
            pltpu.VMEM((2, rows, cols), BF16),
            pltpu.VMEM((rows, cols), BF16),
            pltpu.VMEM((-(-n // 8) * 8, rows), F32),
            pltpu.VMEM((n, -(-n // 8) * 8, rows), F32),
            pltpu.VMEM((rows, 8), F32),
            pltpu.VMEM((rows, 8), F32),
            dma((3,)),
            dma((PIECES,)),
            dma((8,)),
            dma((1,)),
            dma((1,)),
            dma((n, PIECES)),
            dma((1,)),
            dma((n, PIECES)),
            dma((1,)),
            dma((n,)),
            dma((1,)),
            dma((1,)),
            dma((n,)),
            dma((1,)),
            dma((2, n)),
            dma((n,)),
            dma((n, PIECES)),
            dma((1,)),
            dma((n,)),
            dma((1,)),
            dma((1,)),
            dma((1,)),
            dma((PIECES,)),
            dma((1,)),
            dma((n,)),
        ],
        compiler_params=pltpu.CompilerParams(
            collective_id=0, has_side_effects=True, vmem_limit_bytes=60 * 1024 * 1024
        ),
        name="fused_layer",
    )(
        queries,
        keys,
        values,
        lambdas,
        head_gain,
        tokens,
        route_ids.T,
        route_weights.T,
        moe_gain,
        w_gate,
        w_up,
        w_down,
    )
    return pl.pallas_call(
        hand_on_kernel,
        out_shape=tuple(jax.ShapeDtypeStruct(r.shape, r.dtype) for r in results),
        in_specs=[vmem, vmem],
        out_specs=(vmem, vmem),
        compiler_params=pltpu.CompilerParams(vmem_limit_bytes=4 * 1024 * 1024),
        name="hand_on",
    )(*results)


def on_device(
    queries,
    keys,
    values,
    lambdas,
    head_gain,
    tokens,
    route_ids,
    route_weights,
    moe_gain,
    w_gate,
    w_up,
    w_down,
):
    rows = tokens.shape[0]
    expert_count = w_gate.shape[0] * lax.axis_size("ep")
    slots = 2 * rows * route_ids.shape[1] // expert_count
    if w_gate.shape[0] == 1 and lax.axis_size("tp") == lax.axis_size("ep") == 4 and slots >= rows:
        return fused(
            queries, keys, values, lambdas, head_gain, tokens,
            route_ids, route_weights, moe_gain, w_gate, w_up, w_down,
        )
    heads_out = attend(queries, keys, values, lambdas, head_gain)
    expert_out = experts(tokens, route_ids, route_weights, moe_gain, w_gate, w_up, w_down)
    return (heads_out, expert_out)


def solution(mesh):
    in_specs = (
        P(("grp", "ep"), "tp"),
        P(("grp", "ep"), "tp"),
        P(("grp", "ep"), "tp"),
        P("tp"),
        P(),
        P(("grp", "ep"), None),
        P(("grp", "ep"), None),
        P(("grp", "ep"), None),
        P(),
        P("ep", None, "tp"),
        P("ep", None, "tp"),
        P("ep", "tp", None),
    )
    out_specs = (P(("grp", "ep"), "tp"), P(("grp", "ep"), "tp"))
    return jax.shard_map(
        on_device, mesh=mesh, in_specs=in_specs, out_specs=out_specs, check_vma=False
    )
```

```python
import functools

import jax
import jax.numpy as jnp
from jax import lax
from jax.experimental import pallas as pl
from jax.experimental.pallas import tpu as pltpu
from jax.sharding import PartitionSpec as P

MESH = pl.DeviceIdType.MESH
F32 = jnp.float32
BF16 = jnp.bfloat16
PIECES = 4
OUTER_VISIT = 0

def attend(queries, keys, values, lambdas, head_gain):
    row_count = queries.shape[0]
    head_count = lambdas.shape[0]
    head_dim = queries.shape[1] // (2 * head_count)
    value_dim = values.shape[1] // head_count
    query_parts = queries.reshape(row_count, head_count, 2, head_dim)
    score_scale = head_dim ** (-0.5)
    running = jnp.full((head_count, 2, row_count), -1e30, jnp.float32)
    key_piece = lax.all_gather(keys, "ep", axis=0, tiled=True)
    value_piece = lax.all_gather(values, "ep", axis=0, tiled=True)
    count = key_piece.shape[0]
    key_parts = key_piece.reshape(count, head_count, 2, head_dim)
    value_parts = value_piece.reshape(count, head_count, value_dim)
    scores = (
        jnp.einsum("qhcd,khcd->hcqk", query_parts, key_parts, preferred_element_type=jnp.float32)
        * score_scale
    )
    newest = jnp.maximum(running, jnp.max(scores, axis=-1))
    weights_now = jnp.exp(scores - newest[..., None])
    totals = jnp.sum(weights_now, axis=-1)
    sums = jnp.einsum(
        "hcqk,khe->hcqe",
        weights_now.astype(jnp.bfloat16),
        value_parts,
        preferred_element_type=jnp.float32,
    )
    running, totals, sums = (newest, totals, sums)
    means = sums / totals[..., None]
    mixed = means[:, 0] - lambdas[:, None, None] * means[:, 1]
    scaled = mixed * lax.rsqrt(jnp.mean(mixed * mixed, axis=-1, keepdims=True) + 1e-06) * head_gain
    return (
        jnp.transpose(scaled, (1, 0, 2))
        .reshape(row_count, head_count * value_dim)
        .astype(jnp.bfloat16)
    )


def experts(tokens, route_ids, route_weights, moe_gain, w_gate, w_up, w_down):
    row_count, width = tokens.shape
    top_count = route_ids.shape[1]
    ep_size = lax.axis_size("ep")
    tp_size = lax.axis_size("tp")
    expert_count = w_gate.shape[0] * ep_size
    capacity = 2 * row_count * top_count // expert_count
    token_float = tokens.astype(jnp.float32)
    normed = (
        token_float
        * lax.rsqrt(jnp.mean(token_float * token_float, axis=1, keepdims=True) + 1e-06)
        * moe_gain
    ).astype(jnp.bfloat16)
    flat_ids = route_ids.reshape(-1)
    onehot = (flat_ids[:, None] == jnp.arange(expert_count, dtype=jnp.int32)[None, :]).astype(
        jnp.int32
    )
    earlier = jnp.cumsum(onehot, axis=0) - onehot
    position = jnp.sum(earlier * onehot, axis=1)
    slot_index = flat_ids * capacity + position
    owners = (
        jnp.full((expert_count * capacity,), row_count, jnp.int32)
        .at[slot_index]
        .set(jnp.arange(row_count * top_count, dtype=jnp.int32) // top_count)
    )
    padded = jnp.concatenate([normed, jnp.zeros((1, width), jnp.bfloat16)], axis=0)
    outgoing = padded[owners].reshape(expert_count, capacity, width)
    gate_mat = w_gate[0]
    up_mat = w_up[0]
    down_mat = w_down[0]
    slice_width = width // tp_size
    own_columns = lax.dynamic_slice_in_dim(
        outgoing, lax.axis_index("tp") * slice_width, slice_width, 2
    )
    arrived = lax.all_to_all(own_columns, "ep", split_axis=0, concat_axis=0, tiled=True)
    piece = lax.all_gather(arrived, "tp", axis=2, tiled=True)
    gate = jnp.einsum("scd,df->scf", piece, gate_mat, preferred_element_type=jnp.float32)
    upward = jnp.einsum("scd,df->scf", piece, up_mat, preferred_element_type=jnp.float32)
    hidden = (jax.nn.silu(gate) * upward).astype(jnp.bfloat16)
    flat_hidden = hidden.reshape(-1, hidden.shape[2])
    summed = lax.psum_scatter(
        jnp.einsum("fd,sf->ds", down_mat, flat_hidden, preferred_element_type=jnp.float32).astype(
            jnp.bfloat16
        ),
        "tp",
        scatter_dimension=0,
        tiled=True,
    )
    back = lax.all_to_all(summed, "ep", split_axis=1, concat_axis=1, tiled=True)
    picked = (
        jnp.take(back, slot_index, axis=1).astype(jnp.float32).reshape(-1, row_count, top_count)
    )
    combined = jnp.einsum("drk,rk->rd", picked, route_weights)
    return combined.astype(jnp.bfloat16)


def visit_order(n):
    def key(e):
        left = 2 * e < n
        if e in (0, n - 1):
            return lambda s: (False, abs(s - e))
        return lambda s: (s > e if left else s < e, -abs(s - e))

    return [sorted((s for s in range(n) if s != e), key=key(e)) for e in range(n)]


def fused_kernel(
    n,
    q_hbm,
    k_hbm,
    v_hbm,
    lam_hbm,
    hgain_hbm,
    tok_hbm,
    ids_hbm,
    rw_hbm,
    mgain_hbm,
    wg_hbm,
    wu_hbm,
    wd_hbm,
    heads_ref,
    out_ref,
    wg,
    wu,
    wd,
    q_ref,
    lam_ref,
    hgain_ref,
    tok_ref,
    ids_ref,
    rw_ref,
    mgain_ref,
    gathered,
    kv,
    hid,
    part,
    core_in,
    s_own,
    s_out,
    x_in,
    t_out,
    ret,
    z_out,
    z_in,
    join,
    lines,
    tables,
    own_weights,
    weights_at,
    wsem,
    tok_sem,
    in_sem,
    own_send,
    z_send,
    z_recv,
    x_send,
    x_recv,
    c_send,
    c_recv,
    kv_own_send,
    kv_send,
    kv_recv,
    r1_send,
    r1_recv,
    r2_send,
    r2_recv,
    r3_send,
    r3_recv,
    zo_send,
    zo_recv,
    join_send,
    join_recv,
    tab_send,
    tab_recv,
):
    e = lax.axis_index("ep")
    t = lax.axis_index("tp")
    xi = t // 2
    ci = lax.rem(t, 2)
    core_peer = {"tp": 2 * xi + 1 - ci}
    tx = 2 * (1 - xi) + ci
    x_peer = {"tp": tx}
    rows, width = tok_ref.shape
    cols = width // 4
    kv_rows = k_hbm.shape[0]
    has_left = e > 0
    has_right = e < n - 1
    inner = jnp.logical_and(has_left, has_right)
    outer = jnp.logical_not(inner)
    left_half = 2 * e < n
    inward = {"ep": jnp.clip(jnp.where(left_half, e + 1, e - 1), 0, n - 1)}
    outward = {"ep": jnp.clip(jnp.where(left_half, e - 1, e + 1), 0, n - 1)}

    def colblock(j):
        return pl.ds(pl.multiple_of(j * cols, 128), cols)

    def remote(src, dst, ss, rs, dev):
        return pltpu.make_async_remote_copy(
            src_ref=src, dst_ref=dst, send_sem=ss, recv_sem=rs, device_id=dev, device_id_type=MESH
        )

    barrier = pltpu.get_barrier_semaphore()
    pl.semaphore_signal(barrier, inc=1, device_id=inward, device_id_type=MESH)

    @pl.when(inner)
    def _():
        pl.semaphore_signal(barrier, inc=1, device_id=outward, device_id_type=MESH)

    pl.semaphore_signal(barrier, inc=1, device_id=core_peer, device_id_type=MESH)
    pl.semaphore_signal(barrier, inc=1, device_id=x_peer, device_id_type=MESH)
    greeted = 3 + inner.astype(jnp.int32)

    halves = range(PIECES)
    early, late = halves[: PIECES // 2], halves[PIECES // 2 :]
    hr = rows // PIECES

    def half(h):
        return pl.ds(h * hr, hr)

    own_kv = pl.ds(pl.multiple_of(e * kv_rows, kv_rows), kv_rows)
    k_width = k_hbm.shape[1]
    v_width = v_hbm.shape[1]
    gain_in = pltpu.make_async_copy(mgain_hbm, mgain_ref, in_sem.at[0])
    gain_in.start()
    tokens_in = [
        pltpu.make_async_copy(tok_hbm.at[half(h)], tok_ref.at[half(h)], tok_sem.at[h])
        for h in halves
    ]
    for c in tokens_in:
        c.start()
    weights = [
        pltpu.make_async_copy(a, b, wsem.at[i])
        for i, (a, b) in enumerate(((wg_hbm.at[0], wg), (wu_hbm.at[0], wu), (wd_hbm.at[0], wd)))
    ]
    kv_in = [
        pltpu.make_async_copy(k_hbm, kv.at[own_kv, pl.ds(0, k_width)], in_sem.at[1]),
        pltpu.make_async_copy(v_hbm, kv.at[own_kv, pl.ds(k_width, v_width)], in_sem.at[2]),
    ]
    others_in = [
        pltpu.make_async_copy(a, b, in_sem.at[i + 3])
        for i, (a, b) in enumerate(
            ((ids_hbm, ids_ref), (rw_hbm, rw_ref), (q_hbm, q_ref), (lam_hbm, lam_ref), (hgain_hbm, hgain_ref))
        )
    ]

    def normalize(h):
        step = 32

        @pl.loop(0, hr // step)
        def _(i):
            sl = pl.ds(pl.multiple_of(h * hr + i * step, step), step)
            v = tok_ref[sl, :].astype(F32)
            scale = lax.rsqrt(jnp.mean(v * v, axis=1, keepdims=True) + 1e-06)
            gathered[e, sl, :] = (v * scale * mgain_ref[...]).astype(BF16)

    def own_tok(side, h):
        blk = gathered.at[e, half(h), colblock(t)]
        return remote(blk, blk, own_send.at[0], z_recv.at[e, h], (inward, outward)[side])

    def own_tok2(h):
        blk = gathered.at[e, half(h), colblock(tx)]
        return remote(blk, blk, own_send.at[0], x_recv.at[e, h], inward)

    def own_kv_copy(side):
        blk = kv.at[own_kv]
        return remote(blk, blk, kv_own_send.at[0], kv_recv.at[e], (inward, outward)[side])

    orders = visit_order(n)

    def nth(k):
        s = jnp.int32(orders[0][k])
        for i in range(1, n):
            s = jnp.where(e == i, jnp.int32(orders[i][k]), s)
        return s

    visits = [nth(k) for k in range(n - 1)]

    def onward(k):
        return inward if k == OUTER_VISIT else outward

    def z_copy(k, h):
        blk = gathered.at[visits[k], half(h), colblock(t)]
        return remote(blk, blk, z_send.at[0], z_recv.at[visits[k], h], onward(k))

    def kv_copy(k):
        s = visits[k]
        blk = kv.at[pl.ds(pl.multiple_of(s * kv_rows, kv_rows), kv_rows)]
        return remote(blk, blk, kv_send.at[0], kv_recv.at[s], onward(k))

    def x_copy(s, h):
        blk = gathered.at[s, half(h), colblock(t)]
        return remote(blk, blk, x_send.at[0], x_recv.at[s, h], x_peer)

    def c_copy(s, h, which):
        blk = gathered.at[s, half(h), colblock((t, tx)[which])]
        return remote(blk, blk, c_send.at[0], c_recv.at[s], core_peer)

    def r1_copy(s, xx):
        return remote(
            part.at[s, :, colblock(2 * xx + 1 - ci)],
            core_in.at[s, xx],
            r1_send.at[0],
            r1_recv.at[xx, s],
            core_peer,
        )

    def r2_copy(s, h):
        return remote(
            s_out.at[s, half(h)], x_in.at[s, half(h)], r2_send.at[s], r2_recv.at[s, h], x_peer
        )

    def ret_copy(s, h):
        return remote(
            t_out.at[s, half(h)], ret.at[e, half(h)], r3_send.at[0], r3_recv.at[e], {"ep": s}
        )

    def join_copy(s, h):
        return remote(
            t_out.at[s, half(h)], join.at[half(h)], join_send.at[0], join_recv.at[h], inward
        )

    def tab_copy(s):
        return remote(lines, tables.at[e], tab_send.at[0], tab_recv.at[e], {"ep": s})

    def tab_back(s):
        return remote(lines, tables.at[s], tab_send.at[0], tab_recv.at[s], {"ep": s})

    def zo_copy(i, h):
        return remote(
            z_out.at[i, half(h)], z_in.at[i, half(h)], zo_send.at[0], zo_recv.at[0], inward
        )

    ff = wg.shape[1]
    nb = ff // 3

    def up_step(s, b):
        sl = pl.ds(b * nb, nb)
        g = jnp.dot(gathered[s], wg[:, sl], preferred_element_type=F32)
        u = jnp.dot(gathered[s], wu[:, sl], preferred_element_type=F32)
        hid[:, sl] = (g / (1.0 + jnp.exp(-g)) * u).astype(BF16)

    def down_step(s, j):
        sl = colblock(j)
        part[s, :, sl] = jnp.dot(hid[...], wd[:, sl], preferred_element_type=F32).astype(BF16)

    def down_far(s):
        down_step(s, 2 * (1 - xi) + 1 - ci)
        r1_copy(s, 1 - xi).start()
        down_step(s, tx)

    def down_near(s):
        down_step(s, 2 * xi + 1 - ci)
        r1_copy(s, xi).start()
        down_step(s, t)

    def across(s, h):
        return part[s, half(h), colblock(tx)].astype(F32) + core_in[s, 1 - xi, half(h)].astype(F32)

    def along(s, h):
        return part[s, half(h), colblock(t)].astype(F32) + core_in[s, xi, half(h)].astype(F32)

    def exchange(s, h):
        if h == 0:
            r1_copy(s, 1 - xi).wait_recv()
        s_out[s, half(h)] = across(s, h).astype(BF16)
        r2_copy(s, h).start()

    def reduce_z_far(s):
        r1_copy(s, 1 - xi).wait_recv()
        for h in halves:
            z_out[0, half(h)] = across(s, h).astype(BF16)
            zo_copy(0, h).start()

    def reduce_z_near(s):
        r1_copy(s, xi).wait_recv()
        for h in halves:
            z_out[1, half(h)] = along(s, h).astype(BF16)
            zo_copy(1, h).start()

    def take_zo():
        waiter(z_in, zo_send.at[0], zo_recv.at[0]).wait_recv()

    def own_sums():
        r1_copy(e, 1 - xi).wait_recv()
        r1_copy(e, xi).wait_recv()

    def reduce_own(h, joined):
        w = own_weights[half(h), 0:1]
        there = across(e, h) * w
        here = along(e, h) * w
        if joined:
            v = own_weights[half(h), 1:2]
            there = there + z_in[0, half(h)].astype(F32) * v
            here = here + z_in[1, half(h)].astype(F32) * v
        s_out[e, half(h)] = there.astype(BF16)
        r2_copy(e, h).start()
        s_own[half(h)] = here

    def finish(k, h, hand, joined=False):
        s = visits[k]
        if h == 0:
            r1_copy(s, xi).wait_recv()
        r2_copy(s, h).wait_recv()
        total = (along(s, h) + x_in[s, half(h)].astype(F32)) * weights_at[half(h), k : k + 1]
        if joined:
            join_copy(s, h).wait_recv()
            total = total + join[half(h)].astype(F32)
        t_out[s, half(h)] = total.astype(BF16)
        hand(s, h).start()

    def columns(picked):
        pad = jnp.zeros(((-len(picked)) % 8, rows), F32)
        return jnp.concatenate(picked + [pad], axis=0).T

    def line_of(table, x):
        is_x = lax.broadcasted_iota(jnp.int32, table.shape, 0) == x
        return jnp.sum(jnp.where(is_x, table, 0.0), axis=0, keepdims=True)

    def weigh():
        for s in visits:
            tab_back(s).wait_recv()
        weights_at[...] = columns([line_of(tables[s], e) for s in visits])

    def start_table(k):
        tab_copy(visits[k]).start()

    def arrive(k, h, x=True):
        z_copy(k, h).wait_recv()
        if x:
            x_copy(visits[k], h).start()
        c_copy(visits[k], h, 0).start()

    def relay(k, h, x=True):
        z_copy(k, h).wait_recv()
        z_copy(k, h).start()
        if x:
            x_copy(visits[k], h).start()
        c_copy(visits[k], h, 0).start()

    def cross(k, h):
        x_copy(visits[k], h).wait_recv()
        c_copy(visits[k], h, 1).start()

    def waiter(ref, ss, rs):
        return remote(ref, ref, ss, rs, core_peer)

    def ready(s):
        waiter(gathered.at[s, :, pl.ds(0, 2 * cols)], c_send.at[0], c_recv.at[s]).wait_recv()

    def attend(h):
        heads = lam_ref.shape[0]
        vd = v_width // heads
        hd = q_ref.shape[1] // (2 * heads)
        qr = q_ref.shape[0]
        first = lax.broadcasted_iota(jnp.int32, (qr, 2 * hd), 1) < hd
        q = q_ref[:, h * 2 * hd : (h + 1) * 2 * hd].astype(F32)
        both = jnp.concatenate(
            [jnp.where(first, q, 0.0).astype(BF16), jnp.where(first, 0.0, q).astype(BF16)], axis=0
        )
        kh = kv[:, h * 2 * hd : (h + 1) * 2 * hd]
        vh = kv[:, k_width + h * vd : k_width + (h + 1) * vd]
        scores = lax.dot_general(
            both, kh, (((1,), (1,)), ((), ())), preferred_element_type=F32
        ) * (hd ** (-0.5))
        ex = jnp.exp(scores - jnp.max(scores, axis=1, keepdims=True))
        tot = jnp.sum(ex, axis=1, keepdims=True)
        sums = jnp.dot(ex.astype(BF16), vh, preferred_element_type=F32) / tot
        mixed = sums[:qr] - lam_ref[h] * sums[qr:]
        norm = lax.rsqrt(jnp.mean(mixed * mixed, axis=1, keepdims=True) + 1e-06)
        heads_ref[:, h * vd : (h + 1) * vd] = (mixed * norm * hgain_ref[...]).astype(BF16)

    def add_back(k, h, end):
        total = s_own[half(h)] + ret[visits[k], half(h)].astype(F32)
        if end:
            out_ref[half(h), :] = total.astype(BF16)
        else:
            s_own[half(h)] = total

    def drained(k):
        waiter(s_out.at[visits[k]], r2_send.at[visits[k]], r2_recv.at[visits[k], 0]).wait_send()

    def on_inner(fn):
        pl.when(inner)(fn)

    def on_outer(fn):
        pl.when(outer)(fn)

    def at(out, inn):
        if out:

            @on_outer
            def _():
                for f, *args in out:
                    f(*args)

        if inn:

            @on_inner
            def _():
                for f, *args in inn:
                    f(*args)

    def start_kv(side):
        own_kv_copy(side).start()

    def take_kv(k):
        kv_copy(k).wait_recv()

    def pass_kv(k):
        kv_copy(k).wait_recv()
        kv_copy(k).start()

    def start_tok2(h):
        own_tok2(h).start()

    def relays(h):
        relay(OUTER_VISIT, h, False)
        relay(2, h)

    gain_in.wait()
    for c in kv_in + others_in:
        c.start()
    for h in halves:
        if h == 0:
            tokens_in[h].wait()
        normalize(h)
        if h == 0:
            for c in tokens_in[1:]:
                c.wait()
            for c in weights:
                c.start()
            pl.semaphore_wait(barrier, greeted)
        own_tok(0, h).start()

        @on_inner
        def _():
            own_tok(1, h).start()

    for c in kv_in + others_in:
        c.wait()
    ids = ids_ref[...]
    rw = rw_ref[...]
    each = [jnp.sum(jnp.where(ids == x, rw, 0.0), axis=0, keepdims=True) for x in range(n)]
    lines[...] = jnp.concatenate(each + [jnp.zeros((lines.shape[0] - n, rows), F32)], axis=0)
    own_weights[...] = columns([line_of(lines[...], e), line_of(lines[...], visits[OUTER_VISIT])])

    for c in weights:
        c.wait()
    v0, v1, v2 = visits
    up_step(e, 0)
    at([(arrive, 0, 0), (start_tok2, 0)], [(relays, 0)])
    up_step(e, 1)
    at([(arrive, 0, 1), (start_tok2, 1)], [(relays, 1)])
    up_step(e, 2)
    at([(arrive, 0, 2), (start_tok2, 2)], [(relays, 2)])
    down_far(e)
    at(
        [(start_tok2, 3), (arrive, 0, 3), (start_kv, 0), (cross, 0, 0)],
        [(relays, 3), (cross, 0, 0)],
    )
    down_near(e)
    at(
        [
            (arrive, 1, 0), (start_table, 0), (start_table, 1), (cross, 0, 1), (arrive, 1, 1),
            (cross, 0, 2), (arrive, 1, 2),
            (cross, 0, 3),
        ],
        [
            (relay, 1, 0), (start_table, 0), (start_table, 1), (start_table, 2), (cross, 0, 1), (cross, 2, 0), (relay, 1, 1),
            (cross, 0, 2), (cross, 2, 1), (relay, 1, 2), (cross, 0, 3), (cross, 2, 2), (start_kv, 0),
        ],
    )
    ready(v0)
    up_step(v0, 0)
    at([(arrive, 1, 3), (cross, 1, 0)], [(relay, 1, 3), (cross, 2, 3), (start_kv, 1), (cross, 1, 0)])
    up_step(v0, 1)
    at([(arrive, 2, 0), (start_table, 2), (cross, 1, 1)], [(cross, 1, 1)])
    up_step(v0, 2)
    at([(arrive, 2, 1), (cross, 1, 2)], [(cross, 1, 2), (pass_kv, 0)])
    down_far(v0)
    at([(arrive, 2, 2), (cross, 1, 3)], [(cross, 1, 3)])
    down_near(v0)
    own_sums()
    at([(arrive, 2, 3), (reduce_z_far, v0)], [(exchange, v0, 0), (pass_kv, 2), (weigh,)])
    ready(v1)
    up_step(v1, 0)
    at(
        [(reduce_z_near, v0), (cross, 2, 0)],
        [(exchange, v0, 1)],
    )
    up_step(v1, 1)
    at([(cross, 2, 1)], [(exchange, v0, 2)])
    up_step(v1, 2)
    at([(cross, 2, 2)], [(exchange, v0, 3)])
    down_far(v1)
    at([(cross, 2, 3)], [(finish, 0, 0, ret_copy)])
    down_near(v1)
    exchange(v1, 0)
    at([(weigh,)], [(pass_kv, 1)])
    ready(v2)
    up_step(v2, 0)
    exchange(v1, 1)
    at([], [(finish, 0, 1, ret_copy)])
    up_step(v2, 1)
    exchange(v1, 2)
    at([], [(finish, 0, 2, ret_copy)])
    up_step(v2, 2)
    exchange(v1, 3)
    at([], [(finish, 0, 3, ret_copy)])
    down_far(v2)
    at([], [(finish, 1, 0, ret_copy)])
    down_near(v2)
    exchange(v2, 0)
    for h in halves:
        at(
            [(finish, 1, h, join_copy)],
            [(finish, 1, h, ret_copy)] if h else [],
        )
        if h + 1 < PIECES:
            exchange(v2, h + 1)

    def attention():
        for k in range(n - 1):
            take_kv(k)
        for h in range(lam_ref.shape[0]):
            attend(h)

    def attention_here():
        for h in range(lam_ref.shape[0]):
            attend(h)

    at(
        [(finish, 2, h, ret_copy) for h in early] + [(drained, 2)]
        + [(reduce_own, h, False) for h in halves] + [(finish, 2, h, ret_copy) for h in late]
        + [(attention,)],
        [(finish, 2, h, ret_copy, True) for h in early] + [(drained, 2), (take_zo,)]
        + [(reduce_own, h, True) for h in halves]
        + [(finish, 2, h, ret_copy, True) for h in late] + [(attention_here,)],
    )

    for h in halves:
        r2_copy(e, h).wait_recv()
        s_own[half(h)] = s_own[half(h)] + x_in[e, half(h)].astype(F32)

    def gather_back(ks):
        for k in ks:
            waiter(ret.at[visits[k]], r3_send.at[0], r3_recv.at[visits[k]]).wait_recv()
            for h in halves:
                add_back(k, h, k == ks[-1])

    @on_outer
    def _():
        gather_back((0, 1, 2))

    @on_inner
    def _():
        gather_back((2,))

    def sent(ref, sem):
        waiter(ref, sem, c_recv.at[e]).wait_send()

    quarter, double = pl.ds(0, cols), pl.ds(0, 2 * cols)
    sent(part.at[:, :, double], r1_send.at[0])
    sent(gathered.at[pl.ds(0, 3), :, double], c_send.at[0])
    sent(gathered.at[pl.ds(0, 2), :, quarter], own_send.at[0])
    sent(s_out.at[e], r2_send.at[e])
    sent(tables.at[pl.ds(0, 3)], tab_send.at[0])
    sent(s_out.at[v1], r2_send.at[v1])

    @on_outer
    def _():
        sent(gathered.at[pl.ds(0, 3), :, quarter], x_send.at[0])
        sent(z_out, zo_send.at[0])
        sent(kv.at[pl.ds(0, kv_rows)], kv_own_send.at[0])
        sent(t_out.at[0], r3_send.at[0])
        sent(t_out.at[0], join_send.at[0])

    @on_inner
    def _():
        sent(kv.at[pl.ds(0, 2 * kv_rows)], kv_own_send.at[0])
        sent(kv.at[pl.ds(0, 3 * kv_rows)], kv_send.at[0])
        sent(gathered.at[pl.ds(0, 3), :, quarter], z_send.at[0])
        sent(gathered.at[pl.ds(0, 2), :, quarter], x_send.at[0])
        sent(s_out.at[v0], r2_send.at[v0])
        sent(t_out.at[pl.ds(0, 3)], r3_send.at[0])


def hand_on_kernel(a_ref, b_ref, c_ref, d_ref):
    c_ref[...] = a_ref[...]
    d_ref[...] = b_ref[...]


def fused(queries, keys, values, lambdas, head_gain, tokens, route_ids, route_weights, moe_gain, w_gate, w_up, w_down):
    n = lax.axis_size("ep")
    rows, width = tokens.shape
    cols = width // 4
    ff = w_gate.shape[2]
    vmem = pl.BlockSpec(memory_space=pltpu.VMEM)
    hbm = pl.BlockSpec(memory_space=pltpu.HBM)
    dma = pltpu.SemaphoreType.DMA
    results = pl.pallas_call(
        functools.partial(fused_kernel, n),
        out_shape=(
            pltpu.VMEM((queries.shape[0], values.shape[1]), BF16),
            pltpu.VMEM((rows, cols), BF16),
        ),
        in_specs=[hbm] * 12,
        out_specs=(vmem, vmem),
        scratch_shapes=[
            pltpu.VMEM((width, ff), BF16),
            pltpu.VMEM((width, ff), BF16),
            pltpu.VMEM((ff, width), BF16),
            pltpu.VMEM(queries.shape, BF16),
            pltpu.SMEM(lambdas.shape, F32),
            pltpu.VMEM(head_gain.shape, F32),
            pltpu.VMEM((rows, width), BF16),
            pltpu.VMEM(route_ids.shape[::-1], jnp.int32),
            pltpu.VMEM(route_weights.shape[::-1], F32),
            pltpu.VMEM(moe_gain.shape, F32),
            pltpu.VMEM((n, rows, width), BF16),
            pltpu.VMEM((n * keys.shape[0], keys.shape[1] + values.shape[1]), BF16),
            pltpu.VMEM((rows, ff), BF16),
            pltpu.VMEM((n, rows, width), BF16),
            pltpu.VMEM((n, 2, rows, cols), BF16),
            pltpu.VMEM((rows, cols), F32),
            pltpu.VMEM((n, rows, cols), BF16),
            pltpu.VMEM((n, rows, cols), BF16),
            pltpu.VMEM((n, rows, cols), BF16),
            pltpu.VMEM((n, rows, cols), BF16),
            pltpu.VMEM((2, rows, cols), BF16),
            pltpu.VMEM((2, rows, cols), BF16),
            pltpu.VMEM((rows, cols), BF16),
            pltpu.VMEM((-(-n // 8) * 8, rows), F32),
            pltpu.VMEM((n, -(-n // 8) * 8, rows), F32),
            pltpu.VMEM((rows, 8), F32),
            pltpu.VMEM((rows, 8), F32),
            dma((3,)),
            dma((PIECES,)),
            dma((8,)),
            dma((1,)),
            dma((1,)),
            dma((n, PIECES)),
            dma((1,)),
            dma((n, PIECES)),
            dma((1,)),
            dma((n,)),
            dma((1,)),
            dma((1,)),
            dma((n,)),
            dma((1,)),
            dma((2, n)),
            dma((n,)),
            dma((n, PIECES)),
            dma((1,)),
            dma((n,)),
            dma((1,)),
            dma((1,)),
            dma((1,)),
            dma((PIECES,)),
            dma((1,)),
            dma((n,)),
        ],
        compiler_params=pltpu.CompilerParams(
            collective_id=0, has_side_effects=True, vmem_limit_bytes=60 * 1024 * 1024
        ),
        name="fused_layer",
    )(
        queries,
        keys,
        values,
        lambdas,
        head_gain,
        tokens,
        route_ids.T,
        route_weights.T,
        moe_gain,
        w_gate,
        w_up,
        w_down,
    )
    return pl.pallas_call(
        hand_on_kernel,
        out_shape=tuple(jax.ShapeDtypeStruct(r.shape, r.dtype) for r in results),
        in_specs=[vmem, vmem],
        out_specs=(vmem, vmem),
        compiler_params=pltpu.CompilerParams(vmem_limit_bytes=4 * 1024 * 1024),
        name="hand_on",
    )(*results)


def on_device(
    queries,
    keys,
    values,
    lambdas,
    head_gain,
    tokens,
    route_ids,
    route_weights,
    moe_gain,
    w_gate,
    w_up,
    w_down,
):
    rows = tokens.shape[0]
    expert_count = w_gate.shape[0] * lax.axis_size("ep")
    slots = 2 * rows * route_ids.shape[1] // expert_count
    if w_gate.shape[0] == 1 and lax.axis_size("tp") == lax.axis_size("ep") == 4 and slots >= rows:
        return fused(
            queries, keys, values, lambdas, head_gain, tokens,
            route_ids, route_weights, moe_gain, w_gate, w_up, w_down,
        )
    heads_out = attend(queries, keys, values, lambdas, head_gain)
    expert_out = experts(tokens, route_ids, route_weights, moe_gain, w_gate, w_up, w_down)
    return (heads_out, expert_out)


def solution(mesh):
    in_specs = (
        P(("grp", "ep"), "tp"),
        P(("grp", "ep"), "tp"),
        P(("grp", "ep"), "tp"),
        P("tp"),
        P(),
        P(("grp", "ep"), None),
        P(("grp", "ep"), None),
        P(("grp", "ep"), None),
        P(),
        P("ep", None, "tp"),
        P("ep", None, "tp"),
        P("ep", "tp", None),
    )
    out_specs = (P(("grp", "ep"), "tp"), P(("grp", "ep"), "tp"))
    return jax.shard_map(
        on_device, mesh=mesh, in_specs=in_specs, out_specs=out_specs, check_vma=False
    )
```
